256 devices in a mesh: dp: 4 (over y), kv: 32 (over z, x), tp: 2 (over core).
Axes of the slice: x: 4, y: 4, z: 8, core: 2. Of those that a mesh axis runs over, the one named last changes fastest.
Arguments:
- tokens: bfloat16 [1024, 4096], P('dp', ('kv', 'tp')), may hold values from -11.5 to 11.5, as said below
- gain_mix: float32 [4096], replicated, may hold values from 0.1 to 1.9
- gain_mlp: float32 [4096], replicated, may hold values from 0.1 to 1.9
- decay_rate: float32 [16], replicated, may hold values from 0.01 to 1
- w_query: bfloat16 [4096, 1024], P('kv', 'tp'), may hold values from -0.09375 to 0.09375
- w_key: bfloat16 [4096, 1024], P('kv', 'tp'), may hold values from -0.09375 to 0.09375
- w_value: bfloat16 [4096, 2048], P('kv', 'tp'), may hold values from -0.09375 to 0.09375
- w_gate: bfloat16 [4096, 2048], P('kv', 'tp'), may hold values from -0.09375 to 0.09375
- w_mix: bfloat16 [2048, 4096], P('tp', 'kv'), may hold values from -0.125 to 0.125
- w_up: bfloat16 [4096, 16384], P(None, ('kv', 'tp')), may hold values from -0.09375 to 0.09375
- w_down: bfloat16 [16384, 4096], P(('kv', 'tp')), may hold values from -0.125 to 0.125
- state: float32 [1024, 16, 64, 128], P(('dp', 'kv'), 'tp'), may hold values from -2 to 2
Outputs:
- result: bfloat16 [1024, 4096], P('dp', ('kv', 'tp'))
- new_state: float32 [1024, 16, 64, 128], P(('dp', 'kv'), 'tp')
The draws below stay inside these ranges and needn't reach their ends.
Inputs may be any that keep to these rules, and one draw needn't show every extreme that they name: `tokens`: feature scales differ across the features.
All inputs are finite; a program needn't handle non-finite values.
Results may differ from the reference program's by a relative error of at most 0.02.
Values may be sent and summed in bfloat16 or wider, within the bound.
A program may use at most 64 MiB of HBM per device.

```python
import math
import jax
import jax.numpy as jnp
from jax import lax

D = 4096
HEADS = 16
DK = 64
DV = 128
FF = 16384
BATCH = 1024
N_TP = 2


def draw_tokens(key, part):
    col_scale = jnp.exp(jnp.linspace(jnp.log(0.35), jnp.log(2.8), D)).astype(jnp.float32)
    normal_part = jnp.clip(jax.random.normal(key, (BATCH, D), jnp.float32), -4.0, 4.0)
    values_out = normal_part * col_scale[None, :]
    return values_out.astype(jnp.bfloat16)


def spiked(array, stream_key, source, target, parts, factor):
    def block_of(dim):
        return (jnp.arange(array.shape[dim]) // (array.shape[dim] // parts)).reshape((-1,) + (1,) * (array.ndim - 1 - dim))

    near = jax.random.permutation(stream_key, parts)[block_of(target)]
    far = (block_of(target) + parts // 2) % parts
    return jnp.where((block_of(source) == near) | (block_of(source) == far), factor * array, array)


def block_scale(rng, shape, shards, least, largest):
    def one(position, parts):
        heights = jax.random.uniform(jax.random.fold_in(jax.random.fold_in(rng, 6), position), (parts,), jnp.float32, least / len(shards), largest / len(shards))
        return jnp.repeat(jnp.exp(heights), shape[position] // parts).reshape((-1,) + (1,) * (len(shape) - position - 1))

    gain = one(*shards[0])
    for cut in shards[1:]:
        gain = gain * one(*cut)
    return gain


def scatter_about(own_key, shape, deviation, bound, pieces=(), kind=jnp.bfloat16):
    loudness = block_scale(own_key, shape, pieces, -0.22, 0.18) if pieces else 1.0
    drawn = jax.random.normal(own_key, shape, jnp.float32) * deviation * loudness
    return jnp.minimum(jnp.maximum(drawn, -bound), bound).astype(kind)


def noise_with(own_key, shape, width, limit, pieces, heavy, dtype=jnp.bfloat16):
    entries = width * jax.random.normal(own_key, shape, jnp.float32)
    if pieces:
        entries = entries * block_scale(own_key, shape, pieces, -0.22, 0.18)
    return jnp.clip(spiked(entries, jax.random.fold_in(own_key, 3), *heavy), -limit, limit).astype(dtype)


def setup_inputs(seed: int = 0) -> dict:
    key_list = jax.random.split(jax.random.key(seed), 13)
    tokens = draw_tokens(jax.random.fold_in(key_list[12], 71), 0)
    gain_mix = jnp.clip(1.0 + 0.18 * jax.random.normal(key_list[1], (D,), jnp.float32), 0.1, 1.9)
    gain_mlp = jnp.clip(1.0 + 0.18 * jax.random.normal(key_list[2], (D,), jnp.float32), 0.1, 1.9)
    decay_rate = jnp.clip(jnp.exp(jax.random.uniform(key_list[3], (HEADS,), jnp.float32, math.log(0.01), math.log(1.0))), 0.01, 1.0)
    w_query = scatter_about(key_list[4], (D, HEADS * DK), D ** -0.5, 0.09375, ((0, 32), (1, 2)))
    w_key = scatter_about(key_list[5], (D, HEADS * DK), D ** -0.5, 0.09375, ((0, 32), (1, 2)))
    w_value = scatter_about(key_list[6], (D, HEADS * DV), D ** -0.5, 0.09375, ((0, 32), (1, 2)))
    w_gate = scatter_about(key_list[7], (D, HEADS * DV), D ** -0.5, 0.09375, ((0, 32), (1, 2)))
    w_mix = scatter_about(key_list[8], (HEADS * DV, D), (HEADS * DV) ** -0.5, 0.125, ((0, 2), (1, 32)))
    w_up = scatter_about(key_list[9], (D, FF), D ** -0.5, 0.09375, ((1, 64),))
    w_down = noise_with(key_list[10], (FF, D), FF ** -0.5, 0.125, ((0, 64),), (0, 1, 64, 4.0))
    state = scatter_about(key_list[11], (BATCH, HEADS, DK, DV), 0.3, 2.0, ((0, 128), (1, 2)), jnp.float32)
    return {"tokens": tokens, "gain_mix": gain_mix, "gain_mlp": gain_mlp, "decay_rate": decay_rate, "w_query": w_query, "w_key": w_key, "w_value": w_value, "w_gate": w_gate, "w_mix": w_mix, "w_up": w_up, "w_down": w_down, "state": state}


EPS = 1e-06

def reference(tokens, gain_mix, gain_mlp, decay_rate, w_query, w_key, w_value, w_gate, w_mix, w_up, w_down, state):
    batch = tokens.shape[0]
    inputs = tokens.astype(jnp.float32)
    first_scale = lax.rsqrt(lax.optimization_barrier(jnp.mean(inputs * inputs, axis=1, keepdims=True)) + EPS)
    normed = (inputs * first_scale * gain_mix).astype(jnp.bfloat16)
    query = jnp.dot(normed, w_query, preferred_element_type=jnp.float32).astype(jnp.bfloat16)
    keys = jnp.dot(normed, w_key, preferred_element_type=jnp.float32).astype(jnp.bfloat16)
    values = jnp.dot(normed, w_value, preferred_element_type=jnp.float32).astype(jnp.bfloat16)
    gates = jnp.dot(normed, w_gate, preferred_element_type=jnp.float32).astype(jnp.bfloat16)
    query_heads = query.astype(jnp.float32).reshape(batch, HEADS, DK)
    key_heads = keys.astype(jnp.float32).reshape(batch, HEADS, DK) * DK ** (-0.5)
    value_heads = values.astype(jnp.float32).reshape(batch, HEADS, DV)
    gate_heads = gates.astype(jnp.float32).reshape(batch, HEADS, DV)
    decay = jnp.exp(-decay_rate)[None, :, None, None]
    new_state = decay * state + key_heads[:, :, :, None] * value_heads[:, :, None, :]
    read = jnp.einsum('bhd,bhde->bhe', query_heads, new_state, precision=lax.Precision.HIGHEST)
    read = read * lax.rsqrt(lax.optimization_barrier(jnp.mean(read * read, axis=2, keepdims=True)) + EPS)
    heads_out = (jax.nn.silu(gate_heads) * read).reshape(batch, HEADS * DV).astype(jnp.bfloat16)
    group = HEADS * DV // N_TP
    mixed = jnp.zeros((batch, D), jnp.float32)
    for index in range(N_TP):
        product = jnp.dot(heads_out[:, index * group:(index + 1) * group], w_mix[index * group:(index + 1) * group], preferred_element_type=jnp.float32)
        rounded = lax.optimization_barrier(product.astype(jnp.bfloat16))
        mixed = mixed + rounded.astype(jnp.float32)
    resid = (inputs + mixed).astype(jnp.bfloat16)
    resid_f = resid.astype(jnp.float32)
    second_scale = lax.rsqrt(lax.optimization_barrier(jnp.mean(resid_f * resid_f, axis=1, keepdims=True)) + EPS)
    normed_mlp = (resid_f * second_scale * gain_mlp).astype(jnp.bfloat16)
    upper = jnp.dot(normed_mlp, w_up, preferred_element_type=jnp.float32)
    hidden = jnp.square(jax.nn.relu(upper)).astype(jnp.bfloat16)
    down = jnp.dot(hidden, w_down, preferred_element_type=jnp.float32)
    result = (resid_f + down).astype(jnp.bfloat16)
    return (result, new_state)
```

```python
import jax
import jax.numpy as jnp
from jax import lax
from jax.sharding import Mesh
from jax.sharding import PartitionSpec as P
from jax.experimental import pallas as pl
from jax.experimental.pallas import tpu as pltpu

KV = ("kv_0", "kv_1")
KV_TP = ("kv_0", "kv_1", "tp")
DP_KV = ("dp", "kv_0", "kv_1")
EPS = 1e-06
F32 = jnp.float32
BF16 = jnp.bfloat16
MESH = pl.DeviceIdType.MESH
NZ = 8
NX = 4
FAR = (4, 3, 5, 2, 6, 1, 7)


def kernel(
    tokens, gain_mix, gain_mlp, rates, w_query, w_key, w_value, w_gate, w_mix, w_up, w_down, state,
    out, new_state,
    pack, tok_in, tokf, wbuf, wm, wup, wdn, st,
    sbuf, rbuf, ssq_s, ssq_r, rdbuf, hall, pbuf, pin, rg,
    xsb, xrb, zsb, zrb, fsend, frecv, fin,
    loc_sem, ns_sem, tok_ss, tok_rs, w_ss, w_rs, mix_ss, mix_rs, mlp_ss, mlp_rs,
    p1_ss, p1_rs, ssq_ss, ssq_rs, h_ss, h_rs, pr_ss, pr_rs,
    rz_ss, rz_rs, rx_ss, rx_rs, xs_ss, xs_rs, zs_ss, zs_rs, f_ss, f_rs,
):
    z = lax.axis_index("kv_0")
    x = lax.axis_index("kv_1")
    c = lax.axis_index("tp")
    kv = z * NX + x

    def zp(d):
        return lax.rem(z + d, NZ)

    def xp(d):
        return lax.rem(x + d, NX)

    bar = pltpu.get_barrier_semaphore()

    def greet(i, _):
        pl.semaphore_signal(
            bar, inc=1, device_id={"kv_0": zp(i // NX), "kv_1": xp(i % NX)}, device_id_type=MESH
        )
        return 0

    lax.fori_loop(1, NZ * NX, greet, 0)
    for dx in range(NX):
        pl.semaphore_signal(bar, inc=1, device_id={"kv_1": xp(dx), "tp": 1 - c}, device_id_type=MESH)

    def local(src, dst, i):
        cp = pltpu.make_async_copy(src, dst, loc_sem.at[i])
        cp.start()
        return cp

    cq = pl.ds(pl.multiple_of(x * 128, 128), 128)
    cv = pl.ds(pl.multiple_of(x * 256, 256), 256)
    ld_w = [
        local(w_query.at[:, cq], wbuf.at[x, :, 0:128], 0),
        local(w_key.at[:, cq], wbuf.at[x, :, 128:256], 1),
        local(w_value.at[:, cv], wbuf.at[x, :, 256:512], 2),
        local(w_gate.at[:, cv], wbuf.at[x, :, 512:768], 3),
    ]
    ld_st = local(state, st, 4)
    ld_mix = local(w_mix, wm.at[x], 5)
    ld_up = local(w_up, wup.at[c], 6)
    ld_dn = local(w_down, wdn.at[c], 7)

    t32 = tokens[...].astype(F32)
    packed = jnp.concatenate([t32[:128], t32[128:]], axis=1).astype(BF16)
    tok_in[x, c] = packed

    pl.semaphore_wait(bar, 35)

    def remote(src, dst, ss, rs, dev):
        cp = pltpu.make_async_remote_copy(
            src_ref=src, dst_ref=dst, send_sem=ss, recv_sem=rs, device_id=dev, device_id_type=MESH
        )
        cp.start()
        return cp

    tok_cp = []
    for i, (dx, other) in enumerate([(2, 0), (2, 1), (1, 0), (3, 0), (1, 1), (3, 1), (0, 1)]):
        dev = {"kv_1": xp(dx), "tp": (1 - c) if other else c}
        tok_cp.append(remote(tok_in.at[x, c], tok_in.at[x, c], tok_ss.at[i], tok_rs.at[i], dev))

    w_cp = {0: [], 1: [], 2: []}
    for dx in (2, 1, 3):
        dev = {"kv_1": xp(dx)}
        dq = pl.ds(pl.multiple_of(xp(dx) * 128, 128), 128)
        w_cp[0].append(remote(w_query.at[:, dq], wbuf.at[x, :, 0:128], w_ss.at[0, dx], w_rs.at[0, dx], dev))
        w_cp[0].append(remote(w_key.at[:, dq], wbuf.at[x, :, 128:256], w_ss.at[1, dx], w_rs.at[1, dx], dev))
    for j, (w, lo) in enumerate(((w_value, 256), (w_gate, 512))):
        for dx in (2, 1, 3):
            dev = {"kv_1": xp(dx)}
            dv = pl.ds(pl.multiple_of(xp(dx) * 256, 256), 256)
            w_cp[j + 1].append(
                remote(w.at[:, dv], wbuf.at[x, :, lo:lo + 256], w_ss.at[2 + j, dx], w_rs.at[2 + j, dx], dev)
            )

    partner = {"tp": 1 - c}
    mlp_cp = [
        remote(w_up, wup.at[c], mlp_ss.at[0], mlp_rs.at[0], partner),
        remote(w_down, wdn.at[c], mlp_ss.at[1], mlp_rs.at[1], partner),
    ]

    for cp in tok_cp:
        cp.wait_recv()
    low = lax.broadcasted_iota(jnp.int32, (128, 128), 1) < 64
    squares = jnp.zeros((256, 128), F32)
    for xx in range(NX):
        a = tok_in[xx, 0].astype(F32)
        b = tok_in[xx, 1].astype(F32)
        top = jnp.where(low, a, pltpu.roll(b, 64, 1))
        bottom = jnp.where(low, pltpu.roll(a, 64, 1), b)
        both = jnp.concatenate([top, bottom], axis=0)
        tokf[:, :, xx * 128:(xx + 1) * 128] = both.reshape(32, 8, 128)
        squares = squares + both * both
    ssq_s[...] = jnp.broadcast_to(jnp.sum(squares, axis=1, keepdims=True), (256, 128)).reshape(32, 8, 128)
    ssq_cp = []
    for dz in FAR:
        ssq_cp.append(
            remote(ssq_s.at[zp(dz) * NX + x], ssq_r.at[dz], ssq_ss.at[dz], ssq_rs.at[dz], {"kv_0": zp(dz)})
        )
    fz = pl.ds(pl.multiple_of(z * 512, 512), 512)
    normed = (tokf[...].reshape(256, 512) * gain_mix[:, fz]).astype(BF16)

    for ch in range(3):
        for cp in w_cp[ch]:
            cp.wait_recv()
        for ld in (ld_w[0:2], ld_w[2:3], ld_w[3:4])[ch]:
            ld.wait()
        wch = wbuf[:, :, ch * 256:(ch + 1) * 256].reshape(512, 256)
        part = jnp.dot(normed, wch, preferred_element_type=F32).reshape(32, 8, 256)
        sbuf[ch] = jnp.concatenate([part[:, :, :128], part[:, :, 128:]], axis=1).astype(BF16)

        def scatter(i, _, ch=ch):
            zz, xx = zp(i // NX), xp(i % NX)
            remote(
                sbuf.at[ch, zz * NX + xx], rbuf.at[ch, i], p1_ss.at[ch], p1_rs.at[ch], {"kv_0": zz, "kv_1": xx}
            )
            return 0

        lax.fori_loop(1, NZ * NX, scatter, 0)

    mix_cp = []
    for dx in (2, 1, 3):
        mix_cp.append(remote(w_mix, wm.at[x], mix_ss.at[dx], mix_rs.at[dx], {"kv_1": xp(dx)}))

    for cp in ssq_cp:
        cp.wait_recv()
    ssq_r[0] = ssq_s[kv]
    total = jnp.sum(ssq_r[...], axis=0)
    first_scale = lax.rsqrt(total / 4096.0 + EPS)
    scale16 = jnp.concatenate([first_scale, first_scale], axis=0)[None]

    def own(ch):
        pltpu.make_async_copy(rbuf.at[ch, 1:32], rbuf.at[ch, 1:32], p1_rs.at[ch]).wait()
        rbuf[ch, 0] = sbuf[ch, kv]
        summed = jnp.sum(rbuf[ch].astype(F32).reshape(NZ, NX, 16, 128), axis=0)
        return (summed * scale16).astype(BF16).astype(F32)

    qk = own(0)
    qs = qk[:, :8].reshape(32, 128)
    ks = qk[:, 8:].reshape(32, 128) * 0.125
    turned = jnp.transpose(jnp.concatenate([qs, ks, jnp.zeros((64, 128), F32)], axis=0))
    vals = own(1)
    ld_st.wait()
    ns_cp = []
    decays = []
    for dx in range(NX):
        xs = xp(NX - dx)
        pair = []
        for hh in range(2):
            rate = rates[c * 8 + xs * 2 + hh]
            pair.append(jnp.exp(-jnp.full((1, 128), rate, F32)))
        decays.append(pair)
    for b in range(8):
        for dx in range(NX):
            xs = xp(NX - dx)
            for hh in range(2):
                rows = slice(hh * 64, (hh + 1) * 64)
                col = dx * 8 + b
                old = st[b, xs, rows, :]
                new = decays[dx][hh] * old + turned[rows, 32 + col:33 + col] * vals[dx, hh * 8 + b:hh * 8 + b + 1, :]
                st[b, xs, rows, :] = new
                rdbuf[dx, hh * 8 + b:hh * 8 + b + 1, :] = jnp.sum(
                    turned[rows, col:col + 1] * new, axis=0, keepdims=True
                )
        cp = pltpu.make_async_copy(st.at[b], new_state.at[b], ns_sem.at[b])
        cp.start()
        ns_cp.append(cp)
    gates = own(2)
    read = rdbuf[...]
    read = read * lax.rsqrt(jnp.mean(read * read, axis=2, keepdims=True) + EPS)
    heads = (gates / (1.0 + jnp.exp(-gates)) * read).astype(BF16)
    for dx in range(NX):
        hall[z, xp(NX - dx)] = heads[dx]
    h_cp = []
    for dz in FAR:
        h_cp.append(remote(hall.at[z], hall.at[z], h_ss.at[dz], h_rs.at[dz], {"kv_0": zp(dz)}))
    for cp in h_cp:
        cp.wait_recv()
    for cp in mix_cp:
        cp.wait_recv()
    ld_mix.wait()

    pieces = []
    for xs in range(NX):
        both = hall[:, xs].astype(F32)
        for hh in range(2):
            pieces.append(both[:, hh * 8:(hh + 1) * 8].reshape(64, 128).astype(BF16))
    lhs = jnp.concatenate(pieces, axis=1)
    for xx in range(NX):
        prod = jnp.dot(lhs, wm[xx], preferred_element_type=F32).astype(BF16)
        pbuf[0, :, xx * 128:(xx + 1) * 128] = prod[:32]
        pbuf[1, :, xx * 128:(xx + 1) * 128] = prod[32:]
    pr_cp = remote(pbuf.at[1 - c], pin, pr_ss, pr_rs, partner)
    pr_cp.wait_recv()
    mixed = pbuf[c].astype(F32) + pin[...].astype(F32)
    own_tok = []
    for zl in range(4):
        own_tok.append(tokf[(c * 4 + zl) * NX + x])
    rg[x, z] = (jnp.concatenate(own_tok, axis=0) + mixed).astype(BF16)

    rz_cp = {}
    for dz in FAR:
        rz_cp[dz] = remote(rg.at[x, z], rg.at[x, z], rz_ss.at[dz], rz_rs.at[dz], {"kv_0": zp(dz)})
    rx_cp = []
    ORDER = (0, 1, 7, 2, 6, 3, 5, 4)
    for dz in ORDER:
        zz = lax.rem(z - dz + NZ, NZ)
        if dz:
            rz_cp[dz].wait_recv()
        for dx in (2, 1, 3):
            rx_cp.append(
                remote(rg.at[x, zz], rg.at[x, zz], rx_ss.at[dz, dx], rx_rs.at[dz, dx], {"kv_1": xp(dx)})
            )
    ld_up.wait()
    mlp_cp[0].wait_recv()
    acc = [jnp.zeros((128, 256), F32), jnp.zeros((128, 256), F32)]
    squares = jnp.zeros((128, 128), F32)
    for i, dz in enumerate(ORDER):
        zz = lax.rem(z - dz + NZ, NZ)
        for k in range(3):
            rx_cp[i * 3 + k].wait_recv()
        rows = rg[:, zz].reshape(128, 512).astype(F32)
        fk = pl.ds(pl.multiple_of(zz * 512, 512), 512)
        for q in range(4):
            piece = rows[:, q * 128:(q + 1) * 128]
            squares = squares + piece * piece
        lhs = (rows * gain_mlp[:, fk]).astype(BF16)
        for cc in range(2):
            acc[cc] = acc[cc] + jnp.dot(lhs, wup[cc, fk, :], preferred_element_type=F32)
    second_scale = lax.rsqrt(jnp.sum(squares, axis=1, keepdims=True) / 4096.0 + EPS)
    hid = []
    for cc in range(2):
        upper = jnp.maximum(acc[cc] * second_scale, 0.0)
        hid.append((upper * upper).astype(BF16))

    ld_dn.wait()
    mlp_cp[1].wait_recv()
    xs_cp = {}
    for i in range(NZ):
        dz = (FAR + (0,))[i]
        zz = zp(dz)
        fk = pl.ds(pl.multiple_of(zz * 512, 512), 512)
        part = jnp.dot(hid[0], wdn[0, :, fk], preferred_element_type=F32)
        part = part + jnp.dot(hid[1], wdn[1, :, fk], preferred_element_type=F32)
        part = part.astype(BF16)
        for xx in range(NX):
            xsb[dz, xx] = part[:, xx * 128:(xx + 1) * 128]
        for dx in (2, 1, 3):
            xs_cp[dz, dx] = remote(
                xsb.at[dz, xp(dx)], xrb.at[dz, dx - 1], xs_ss.at[dz, dx], xs_rs.at[dz, dx], {"kv_1": xp(dx)}
            )
    zs_cp = {}
    own_sum = None
    for i in range(NZ):
        dz = (FAR + (0,))[i]
        for dx in (2, 1, 3):
            xs_cp[dz, dx].wait_recv()
        summed = xsb[dz, x].astype(F32) + jnp.sum(xrb[dz].astype(F32), axis=0)
        if dz:
            zsb[dz] = summed.astype(BF16)
            zs_cp[dz] = remote(zsb.at[dz], zrb.at[dz - 1], zs_ss.at[dz], zs_rs.at[dz], {"kv_0": zp(dz)})
        else:
            own_sum = summed
    for dz in FAR:
        zs_cp[dz].wait_recv()
    down = own_sum + jnp.sum(zrb[...].astype(F32), axis=0)
    lanes = pl.ds(pl.multiple_of(x * 128, 128), 128)
    res = rg[:, z, :, lanes].reshape(128, 128).astype(F32)
    fsend[...] = (res + down).astype(BF16)
    f_cp = remote(fsend, frecv, f_ss, f_rs, partner)
    f_cp.wait_recv()
    for who, ref in ((c, fsend), (1 - c, frecv)):
        block = ref[...].astype(F32)
        for xs in range(NX):
            for zl in range(4):
                r0 = xs * 32 + zl * 8
                fin[(who * 4 + zl) * NX + xs] = block[r0:r0 + 8]
    done = fin[...].reshape(256, 128)
    out[...] = jnp.where(c == 0, done, pltpu.roll(done, 64, 1))[:, :64].astype(BF16)

    for cp in tok_cp + w_cp[0] + w_cp[1] + w_cp[2] + mlp_cp + ssq_cp + mix_cp + h_cp + [pr_cp]:
        cp.wait_send()
    for ch in range(3):
        pltpu.make_async_copy(sbuf.at[ch, 1:32], sbuf.at[ch, 1:32], p1_ss.at[ch]).wait()
    for cp in list(rz_cp.values()) + rx_cp + list(xs_cp.values()) + list(zs_cp.values()) + [f_cp]:
        cp.wait_send()
    for cp in ns_cp:
        cp.wait()


def per_device(
    tokens, gain_mix, gain_mlp, decay_rate, w_query, w_key, w_value, w_gate, w_mix, w_up, w_down, state
):
    vm = pl.BlockSpec(memory_space=pltpu.VMEM)
    hbm = pl.BlockSpec(memory_space=pltpu.HBM)
    dma = pltpu.SemaphoreType.DMA
    result, new_state = pl.pallas_call(
        kernel,
        out_shape=(
            jax.ShapeDtypeStruct((256, 64), BF16),
            jax.ShapeDtypeStruct((8, 4, 128, 128), F32),
        ),
        in_specs=[vm, vm, vm, pl.BlockSpec(memory_space=pltpu.SMEM)] + [hbm] * 8,
        out_specs=(vm, hbm),
        scratch_shapes=[
            pltpu.VMEM((128, 128), BF16),
            pltpu.VMEM((4, 2, 128, 128), BF16),
            pltpu.VMEM((32, 8, 512), F32),
            pltpu.VMEM((4, 128, 768), BF16),
            pltpu.VMEM((4, 1024, 128), BF16),
            pltpu.VMEM((2, 4096, 256), BF16),
            pltpu.VMEM((2, 256, 4096), BF16),
            pltpu.VMEM((8, 4, 128, 128), F32),
            pltpu.VMEM((3, 32, 16, 128), BF16),
            pltpu.VMEM((3, 32, 16, 128), BF16),
            pltpu.VMEM((32, 8, 128), F32),
            pltpu.VMEM((8, 8, 128), F32),
            pltpu.VMEM((4, 16, 128), F32),
            pltpu.VMEM((8, 4, 16, 128), BF16),
            pltpu.VMEM((2, 32, 512), BF16),
            pltpu.VMEM((32, 512), BF16),
            pltpu.VMEM((4, 8, 32, 512), BF16),
            pltpu.VMEM((8, 4, 128, 128), BF16),
            pltpu.VMEM((8, 3, 128, 128), BF16),
            pltpu.VMEM((8, 128, 128), BF16),
            pltpu.VMEM((7, 128, 128), BF16),
            pltpu.VMEM((128, 128), BF16),
            pltpu.VMEM((128, 128), BF16),
            pltpu.VMEM((32, 8, 128), F32),
            dma((8,)), dma((8,)), dma((7,)), dma((7,)), dma((4, 4)), dma((4, 4)), dma((4,)), dma((4,)),
            dma((2,)), dma((2,)), dma((3,)), dma((3,)), dma((8,)), dma((8,)), dma((8,)), dma((8,)),
            dma, dma, dma((8,)), dma((8,)), dma((8, 4)), dma((8, 4)), dma((8, 4)), dma((8, 4)),
            dma((8,)), dma((8,)), dma, dma,
        ],
        compiler_params=pltpu.CompilerParams(
            collective_id=0, has_side_effects=True, vmem_limit_bytes=60 * 1024 * 1024
        ),
        name="layer",
    )(
        tokens, gain_mix.reshape(1, 4096), gain_mlp.reshape(1, 4096), decay_rate,
        w_query, w_key, w_value, w_gate, w_mix, w_up, w_down, state.reshape(8, 4, 128, 128),
    )
    return result, new_state.reshape(8, 8, 64, 128)


def solution(mesh):
    torus = Mesh(
        mesh.devices.reshape(mesh.shape["dp"], 8, 4, mesh.shape["tp"]), ("dp", "kv_0", "kv_1", "tp")
    )
    return jax.shard_map(
        per_device,
        mesh=torus,
        in_specs=(
            P("dp", KV_TP),
            P(),
            P(),
            P(),
            P(KV, "tp"),
            P(KV, "tp"),
            P(KV, "tp"),
            P(KV, "tp"),
            P("tp", KV),
            P(None, KV_TP),
            P(KV_TP, None),
            P(DP_KV, "tp", None, None),
        ),
        out_specs=(P("dp", KV_TP), P(DP_KV, "tp", None, None)),
        check_vma=False,
    )
```

```python
import jax
import jax.numpy as jnp
from jax import lax
from jax.sharding import Mesh
from jax.sharding import PartitionSpec as P
from jax.experimental import pallas as pl
from jax.experimental.pallas import tpu as pltpu

KV = ("kv_0", "kv_1")
KV_TP = ("kv_0", "kv_1", "tp")
DP_KV = ("dp", "kv_0", "kv_1")
EPS = 1e-06
F32 = jnp.float32
BF16 = jnp.bfloat16
MESH = pl.DeviceIdType.MESH
NZ = 8
NX = 4
FAR = (4, 3, 5, 2, 6, 1, 7)


def kernel(
    tokens, gain_mix_h, gain_mlp_h, rates, w_query, w_key, w_value, w_gate, w_mix, w_up, w_down, state,
    out, keys_out, vals_out,
    gain_mix, gain_mlp, tok_in, tokf, wbuf, wm, wup, wdn, st,
    sbuf, rbuf, ssq_s, ssq_r, qk_abs, v_abs, g_abs, rdbuf, hall, pbuf, pin, rg,
    xsb, xrb, zsb, zrb, fsend, frecv, fin, fint,
    loc_sem, tok_ss, tok_rs, w_ss, w_rs, mix_ss, mix_rs, my_ss, my_rs, mlp_ss, mlp_rs,
    p1_ss, p1_rs, ssq_ss, ssq_rs, h_ss, h_rs, pr_ss, pr_rs,
    rz_ss, rz_rs, rx_ss, rx_rs, xs_ss, xs_rs, zs_ss, zs_rs, f_ss, f_rs,
):
    z = lax.axis_index("kv_0")
    x = lax.axis_index("kv_1")
    c = lax.axis_index("tp")
    y = lax.axis_index("dp")
    kv = z * NX + x

    def zp(d):
        return lax.rem(z + d, NZ)

    def xp(d):
        return lax.rem(x + d, NX)

    bar = pltpu.get_barrier_semaphore()

    def greet(i, _):
        pl.semaphore_signal(
            bar, inc=1, device_id={"kv_0": zp(i // NX), "kv_1": xp(i % NX)}, device_id_type=MESH
        )
        return 0

    lax.fori_loop(1, NZ * NX, greet, 0)
    for dx in range(NX):
        pl.semaphore_signal(bar, inc=1, device_id={"kv_1": xp(dx), "tp": 1 - c}, device_id_type=MESH)
    for dy in range(1, 4):
        pl.semaphore_signal(bar, inc=1, device_id={"dp": lax.rem(y + dy, 4)}, device_id_type=MESH)

    def local(src, dst, i):
        cp = pltpu.make_async_copy(src, dst, loc_sem.at[i])
        cp.start()
        return cp

    cq = pl.ds(pl.multiple_of(x * 128, 128), 128)
    cv = pl.ds(pl.multiple_of(x * 256, 256), 256)
    ld_tok = local(tokens, tok_in.at[x, c], 8)
    ld_gains = [local(gain_mix_h, gain_mix, 9), local(gain_mlp_h, gain_mlp, 10)]
    ld_w = [
        local(w_query.at[:, cq], wbuf.at[x, :, 0:128], 0),
        local(w_key.at[:, cq], wbuf.at[x, :, 128:256], 1),
        local(w_value.at[:, cv], wbuf.at[x, :, 256:512], 2),
        local(w_gate.at[:, cv], wbuf.at[x, :, 512:768], 3),
    ]
    ld_st = local(state, st, 4)
    ld_mix = local(w_mix, wm.at[x], 5)
    ld_up = local(w_up, wup.at[c], 6)
    ld_dn = local(w_down, wdn.at[c], 7)

    ld_tok.wait()
    pl.semaphore_wait(bar, 38)

    def remote(src, dst, ss, rs, dev):
        cp = pltpu.make_async_remote_copy(
            src_ref=src, dst_ref=dst, send_sem=ss, recv_sem=rs, device_id=dev, device_id_type=MESH
        )
        cp.start()
        return cp

    tok_cp = []
    for i, (dx, other) in enumerate([(2, 0), (2, 1), (1, 0), (3, 0), (1, 1), (3, 1), (0, 1)]):
        dev = {"kv_1": xp(dx), "tp": (1 - c) if other else c}
        tok_cp.append(remote(tok_in.at[x, c], tok_in.at[x, c], tok_ss.at[i], tok_rs.at[i], dev))

    w_cp = {0: [], 1: [], 2: []}
    for dx in (2, 1, 3):
        dev = {"kv_1": xp(dx)}
        dq = pl.ds(pl.multiple_of(xp(dx) * 128, 128), 128)
        w_cp[0].append(remote(w_query.at[:, dq], wbuf.at[x, :, 0:128], w_ss.at[0, dx], w_rs.at[0, dx], dev))
        w_cp[0].append(remote(w_key.at[:, dq], wbuf.at[x, :, 128:256], w_ss.at[1, dx], w_rs.at[1, dx], dev))
    for j, (w, lo) in enumerate(((w_value, 256), (w_gate, 512))):
        for dx in (2, 1, 3):
            dev = {"kv_1": xp(dx)}
            dv = pl.ds(pl.multiple_of(xp(dx) * 256, 256), 256)
            w_cp[j + 1].append(
                remote(w.at[:, dv], wbuf.at[x, :, lo:lo + 256], w_ss.at[2 + j, dx], w_rs.at[2 + j, dx], dev)
            )

    partner = {"tp": 1 - c}
    mlp_cp = [
        remote(w_up, wup.at[c], mlp_ss.at[0], mlp_rs.at[0], partner),
        remote(w_down, wdn.at[c], mlp_ss.at[1], mlp_rs.at[1], partner),
    ]

    for cp in tok_cp:
        cp.wait_recv()
    squares = jnp.zeros((256, 128), F32)
    for xx in range(NX):
        both = jnp.transpose(tok_in[xx].reshape(128, 256).astype(F32))
        tokf[:, :, xx * 128:(xx + 1) * 128] = both.reshape(32, 8, 128)
        squares = squares + both * both
    ssq_s[...] = jnp.broadcast_to(jnp.sum(squares, axis=1, keepdims=True), (256, 128)).reshape(32, 8, 128)
    ssq_cp = []
    for dz in FAR:
        ssq_cp.append(
            remote(ssq_s.at[zp(dz) * NX + x], ssq_r.at[dz], ssq_ss.at[dz], ssq_rs.at[dz], {"kv_0": zp(dz)})
        )
    fz = pl.ds(pl.multiple_of(z * 512, 512), 512)
    for ld in ld_gains:
        ld.wait()
    normed = (tokf[...].reshape(256, 512) * gain_mix[:, fz]).astype(BF16)

    for ch in range(3):
        for cp in w_cp[ch]:
            cp.wait_recv()
        for ld in (ld_w[0:2], ld_w[2:3], ld_w[3:4])[ch]:
            ld.wait()
        wch = wbuf[:, :, ch * 256:(ch + 1) * 256].reshape(512, 256)
        part = jnp.dot(normed, wch, preferred_element_type=F32).reshape(32, 8, 256)
        sbuf[ch] = jnp.concatenate([part[:, :, :128], part[:, :, 128:]], axis=1).astype(BF16)

        def scatter(i, _, ch=ch):
            zz, xx = zp(i // NX), xp(i % NX)
            remote(
                sbuf.at[ch, zz * NX + xx], rbuf.at[ch, i], p1_ss.at[ch], p1_rs.at[ch], {"kv_0": zz, "kv_1": xx}
            )
            return 0

        lax.fori_loop(1, NZ * NX, scatter, 0)

    qrows = pl.ds(pl.multiple_of(y * 256, 256), 256)
    mix_cp = []
    for dx in (2, 1, 3):
        mix_cp.append(
            remote(w_mix.at[qrows], wm.at[x, qrows], mix_ss.at[dx], mix_rs.at[dx], {"kv_1": xp(dx)})
        )

    for cp in ssq_cp:
        cp.wait_recv()
    ssq_r[0] = ssq_s[kv]
    total = jnp.sum(ssq_r[...], axis=0)
    first_scale = lax.rsqrt(total / 4096.0 + EPS)
    scale16 = jnp.concatenate([first_scale, first_scale], axis=0)[None]

    def own(ch):
        pltpu.make_async_copy(rbuf.at[ch, 1:32], rbuf.at[ch, 1:32], p1_rs.at[ch]).wait()
        rbuf[ch, 0] = sbuf[ch, kv]
        summed = jnp.sum(rbuf[ch].astype(F32).reshape(NZ, NX, 16, 128), axis=0)
        return (summed * scale16).astype(BF16).astype(F32)

    qk = own(0)
    for dx in range(NX):
        qk_abs[xp(NX - dx)] = qk[dx]
    vals = own(1)
    for dx in range(NX):
        v_abs[xp(NX - dx)] = vals[dx]
    my_cp = []
    for i, dx in enumerate((2, 1, 3)):
        mix_cp[i].wait_recv()
        src = wm.at[xp(NX - dx), qrows]
        for dy in (2, 1, 3):
            my_cp.append(remote(src, src, my_ss.at[dx, dy], my_rs.at[dx, dy], {"dp": lax.rem(y + dy, 4)}))
    qs = qk_abs[:, :8].reshape(32, 128)
    ks = qk_abs[:, 8:].reshape(32, 128) * 0.125
    turned = jnp.transpose(jnp.concatenate([qs, ks, jnp.zeros((64, 128), F32)], axis=0))
    keys_out[...] = turned
    vals_out[...] = v_abs[...]
    ld_st.wait()
    decays = [jnp.exp(-jnp.full((1, 128), rates[c * 8 + h], F32)) for h in range(8)]
    for xs in range(NX):
        for b in range(8):
            for hh in range(2):
                rows = slice(hh * 64, (hh + 1) * 64)
                col = xs * 8 + b
                new = decays[xs * 2 + hh] * st[b, xs, rows, :] + (
                    turned[rows, 32 + col:33 + col] * v_abs[xs, hh * 8 + b:hh * 8 + b + 1, :]
                )
                rdbuf[xs, hh * 8 + b:hh * 8 + b + 1, :] = jnp.sum(
                    turned[rows, col:col + 1] * new, axis=0, keepdims=True
                )
    gates = own(2)
    for dx in range(NX):
        g_abs[xp(NX - dx)] = gates[dx]
    gates = g_abs[...]
    read = rdbuf[...]
    read = read * lax.rsqrt(jnp.mean(read * read, axis=2, keepdims=True) + EPS)
    hall[z] = (gates / (1.0 + jnp.exp(-gates)) * read).astype(BF16)
    h_cp = []
    for dz in FAR:
        h_cp.append(remote(hall.at[z], hall.at[z], h_ss.at[dz], h_rs.at[dz], {"kv_0": zp(dz)}))
    for cp in h_cp:
        cp.wait_recv()
    for cp in my_cp:
        cp.wait_recv()
    ld_mix.wait()

    pieces = []
    for xs in range(NX):
        both = hall[:, xs].astype(F32)
        for hh in range(2):
            pieces.append(both[:, hh * 8:(hh + 1) * 8].reshape(64, 128).astype(BF16))
    lhs = jnp.concatenate(pieces, axis=1)
    for xx in range(NX):
        prod = jnp.dot(lhs, wm[xx], preferred_element_type=F32).astype(BF16)
        pbuf[0, :, xx * 128:(xx + 1) * 128] = prod[:32]
        pbuf[1, :, xx * 128:(xx + 1) * 128] = prod[32:]
    pr_cp = remote(pbuf.at[1 - c], pin, pr_ss, pr_rs, partner)
    pr_cp.wait_recv()
    mixed = pbuf[c].astype(F32) + pin[...].astype(F32)
    own_tok = []
    for zl in range(4):
        own_tok.append(tokf[(c * 4 + zl) * NX + x])
    rg[x, z] = (jnp.concatenate(own_tok, axis=0) + mixed).astype(BF16)

    rz_cp = {}
    for dz in (1, 7, 2, 6, 3, 5, 4):
        rz_cp[dz] = remote(rg.at[x, z], rg.at[x, z], rz_ss.at[dz], rz_rs.at[dz], {"kv_0": zp(dz)})
    rx_cp = []
    ORDER = (0, 1, 7, 2, 6, 3, 5, 4)
    for dz in ORDER:
        zz = lax.rem(z - dz + NZ, NZ)
        if dz:
            rz_cp[dz].wait_recv()
        for dx in (2, 1, 3):
            rx_cp.append(
                remote(rg.at[x, zz], rg.at[x, zz], rx_ss.at[dz, dx], rx_rs.at[dz, dx], {"kv_1": xp(dx)})
            )
    ld_up.wait()
    mlp_cp[0].wait_recv()
    acc = [jnp.zeros((128, 256), F32), jnp.zeros((128, 256), F32)]
    squares = jnp.zeros((128, 128), F32)
    for i, dz in enumerate(ORDER):
        zz = lax.rem(z - dz + NZ, NZ)
        for k in range(3):
            rx_cp[i * 3 + k].wait_recv()
        rows = rg[:, zz].reshape(128, 512).astype(F32)
        fk = pl.ds(pl.multiple_of(zz * 512, 512), 512)
        for q in range(4):
            piece = rows[:, q * 128:(q + 1) * 128]
            squares = squares + piece * piece
        lhs = (rows * gain_mlp[:, fk]).astype(BF16)
        for cc in range(2):
            acc[cc] = acc[cc] + jnp.dot(lhs, wup[cc, fk, :], preferred_element_type=F32)
    second_scale = lax.rsqrt(jnp.sum(squares, axis=1, keepdims=True) / 4096.0 + EPS)
    hid = []
    for cc in range(2):
        upper = jnp.maximum(acc[cc] * second_scale, 0.0)
        hid.append((upper * upper).astype(BF16))

    ld_dn.wait()
    mlp_cp[1].wait_recv()
    xs_cp = {}
    for i in range(NZ):
        dz = (FAR + (0,))[i]
        zz = zp(dz)
        fk = pl.ds(pl.multiple_of(zz * 512, 512), 512)
        part = jnp.dot(hid[0], wdn[0, :, fk], preferred_element_type=F32)
        part = part + jnp.dot(hid[1], wdn[1, :, fk], preferred_element_type=F32)
        part = part.astype(BF16)
        for xx in range(NX):
            xsb[dz, xx] = part[:, xx * 128:(xx + 1) * 128]
        for dx in (2, 1, 3):
            xs_cp[dz, dx] = remote(
                xsb.at[dz, xp(dx)], xrb.at[dz, dx - 1], xs_ss.at[dz, dx], xs_rs.at[dz, dx], {"kv_1": xp(dx)}
            )
    zs_cp = {}
    own_sum = None
    for i in range(NZ):
        dz = (FAR + (0,))[i]
        for dx in (2, 1, 3):
            xs_cp[dz, dx].wait_recv()
        summed = xsb[dz, x].astype(F32) + jnp.sum(xrb[dz].astype(F32), axis=0)
        if dz:
            zsb[dz] = summed.astype(BF16)
            zs_cp[dz] = remote(zsb.at[dz], zrb.at[dz - 1], zs_ss.at[dz], zs_rs.at[dz], {"kv_0": zp(dz)})
        else:
            own_sum = summed
    for dz in FAR:
        zs_cp[dz].wait_recv()
    down = own_sum + jnp.sum(zrb[...].astype(F32), axis=0)
    lanes = pl.ds(pl.multiple_of(x * 128, 128), 128)
    res = rg[:, z, :, lanes].reshape(128, 128).astype(F32)
    fsend[...] = (res + down).astype(BF16)
    f_cp = remote(fsend, frecv, f_ss, f_rs, partner)
    f_cp.wait_recv()
    for who, ref in ((c, fsend), (1 - c, frecv)):
        block = ref[...].astype(F32)
        for xs in range(NX):
            for zl in range(4):
                r0 = xs * 32 + zl * 8
                fin[(who * 4 + zl) * NX + xs] = block[r0:r0 + 8]
    fint[...] = jnp.transpose(fin[...].reshape(256, 128))
    out[...] = fint[pl.ds(pl.multiple_of(c * 64, 64), 64), :].astype(BF16)

    for cp in tok_cp + w_cp[0] + w_cp[1] + w_cp[2] + mlp_cp + ssq_cp + mix_cp + my_cp + h_cp + [pr_cp]:
        cp.wait_send()
    for ch in range(3):
        pltpu.make_async_copy(sbuf.at[ch, 1:32], sbuf.at[ch, 1:32], p1_ss.at[ch]).wait()
    for cp in list(rz_cp.values()) + rx_cp + list(xs_cp.values()) + list(zs_cp.values()) + [f_cp]:
        cp.wait_send()


def tail(rates, keys, vals, res_in, state, result, new_state, st, ld_sem, out_sem):
    c = lax.axis_index("tp")
    loads = [pltpu.make_async_copy(state.at[b], st.at[b], ld_sem.at[b]) for b in range(8)]
    for cp in loads:
        cp.start()
    result[...] = res_in[...]
    decays = [jnp.exp(-jnp.full((1, 128), rates[c * 8 + h], F32)) for h in range(8)]
    stores = []
    for b in range(8):
        loads[b].wait()
        for xs in range(NX):
            for hh in range(2):
                rows = slice(hh * 64, (hh + 1) * 64)
                col = 32 + xs * 8 + b
                st[b, xs, rows, :] = decays[xs * 2 + hh] * st[b, xs, rows, :] + (
                    keys[rows, col:col + 1] * vals[xs, hh * 8 + b:hh * 8 + b + 1, :]
                )
        cp = pltpu.make_async_copy(st.at[b], new_state.at[b], out_sem.at[b])
        cp.start()
        stores.append(cp)
    for cp in stores:
        cp.wait()


def per_device(
    tokens, gain_mix, gain_mlp, decay_rate, w_query, w_key, w_value, w_gate, w_mix, w_up, w_down, state
):
    vm = pl.BlockSpec(memory_space=pltpu.VMEM)
    sm = pl.BlockSpec(memory_space=pltpu.SMEM)
    hbm = pl.BlockSpec(memory_space=pltpu.HBM)
    dma = pltpu.SemaphoreType.DMA
    state = state.reshape(8, 4, 128, 128)
    result, keys, vals = pl.pallas_call(
        kernel,
        out_shape=(
            jax.ShapeDtypeStruct((64, 256), BF16),
            jax.ShapeDtypeStruct((128, 128), F32),
            jax.ShapeDtypeStruct((4, 16, 128), F32),
        ),
        in_specs=[hbm, hbm, hbm, sm] + [hbm] * 8,
        out_specs=(vm, vm, vm),
        scratch_shapes=[
            pltpu.VMEM((1, 4096), F32),
            pltpu.VMEM((1, 4096), F32),
            pltpu.VMEM((4, 2, 64, 256), BF16),
            pltpu.VMEM((32, 8, 512), F32),
            pltpu.VMEM((4, 128, 768), BF16),
            pltpu.VMEM((4, 1024, 128), BF16),
            pltpu.VMEM((2, 4096, 256), BF16),
            pltpu.VMEM((2, 256, 4096), BF16),
            pltpu.VMEM((8, 4, 128, 128), F32),
            pltpu.VMEM((3, 32, 16, 128), BF16),
            pltpu.VMEM((3, 32, 16, 128), BF16),
            pltpu.VMEM((32, 8, 128), F32),
            pltpu.VMEM((8, 8, 128), F32),
            pltpu.VMEM((4, 16, 128), F32),
            pltpu.VMEM((4, 16, 128), F32),
            pltpu.VMEM((4, 16, 128), F32),
            pltpu.VMEM((4, 16, 128), F32),
            pltpu.VMEM((8, 4, 16, 128), BF16),
            pltpu.VMEM((2, 32, 512), BF16),
            pltpu.VMEM((32, 512), BF16),
            pltpu.VMEM((4, 8, 32, 512), BF16),
            pltpu.VMEM((8, 4, 128, 128), BF16),
            pltpu.VMEM((8, 3, 128, 128), BF16),
            pltpu.VMEM((8, 128, 128), BF16),
            pltpu.VMEM((7, 128, 128), BF16),
            pltpu.VMEM((128, 128), BF16),
            pltpu.VMEM((128, 128), BF16),
            pltpu.VMEM((32, 8, 128), F32),
            pltpu.VMEM((128, 256), F32),
            dma((11,)), dma((7,)), dma((7,)), dma((4, 4)), dma((4, 4)), dma((4,)), dma((4,)), dma((4, 4)), dma((4, 4)),
            dma((2,)), dma((2,)), dma((3,)), dma((3,)), dma((8,)), dma((8,)), dma((8,)), dma((8,)),
            dma, dma, dma((8,)), dma((8,)), dma((8, 4)), dma((8, 4)), dma((8, 4)), dma((8, 4)),
            dma((8,)), dma((8,)), dma, dma,
        ],
        compiler_params=pltpu.CompilerParams(
            collective_id=0, has_side_effects=True, vmem_limit_bytes=60 * 1024 * 1024
        ),
        name="layer",
    )(
        tokens.T, gain_mix.reshape(1, 4096), gain_mlp.reshape(1, 4096), decay_rate,
        w_query, w_key, w_value, w_gate, w_mix, w_up, w_down, state,
    )
    result, new_state = pl.pallas_call(
        tail,
        out_shape=(
            jax.ShapeDtypeStruct((64, 256), BF16),
            jax.ShapeDtypeStruct((8, 4, 128, 128), F32),
        ),
        in_specs=[sm, vm, vm, vm, hbm],
        out_specs=(vm, hbm),
        scratch_shapes=[pltpu.VMEM((8, 4, 128, 128), F32), dma((8,)), dma((8,))],
        name="tail",
    )(decay_rate, keys, vals, result, state)
    return result.T, new_state.reshape(8, 8, 64, 128)


def solution(mesh):
    torus = Mesh(
        mesh.devices.reshape(mesh.shape["dp"], 8, 4, mesh.shape["tp"]), ("dp", "kv_0", "kv_1", "tp")
    )
    return jax.shard_map(
        per_device,
        mesh=torus,
        in_specs=(
            P("dp", KV_TP),
            P(),
            P(),
            P(),
            P(KV, "tp"),
            P(KV, "tp"),
            P(KV, "tp"),
            P(KV, "tp"),
            P("tp", KV),
            P(None, KV_TP),
            P(KV_TP, None),
            P(DP_KV, "tp", None, None),
        ),
        out_specs=(P("dp", KV_TP), P(DP_KV, "tp", None, None)),
        check_vma=False,
    )
```

```python
import jax
import jax.numpy as jnp
from jax import lax
from jax.sharding import Mesh
from jax.sharding import PartitionSpec as P
from jax.experimental import pallas as pl
from jax.experimental.pallas import tpu as pltpu

KV = ("kv_0", "kv_1")
KV_TP = ("kv_0", "kv_1", "tp")
DP_KV = ("dp", "kv_0", "kv_1")
EPS = 1e-06
F32 = jnp.float32
BF16 = jnp.bfloat16
MESH = pl.DeviceIdType.MESH
NZ = 8
NX = 4
FAR = (4, 3, 5, 2, 6, 1, 7)


def kernel(
    tokens, gain_mix_h, gain_mlp_h, rates, w_query, w_key, w_value, w_gate, w_mix, w_up, w_down, state,
    out, keys_out, vals_out,
    gain_mix, gain_mlp, tok_in, tokf, wbuf, wm, wup, wdn, st,
    sbuf, rbuf, ssq_s, ssq_r, qk_abs, v_abs, g_abs, rdbuf, hall, pbuf, pin, rg,
    xsb, xrb, zsb, zrb, fsend, frecv, fin, fint,
    loc_sem, tok_ss, tok_rs, w_ss, w_rs, mix_ss, mix_rs, my_ss, my_rs, mlp_ss, mlp_rs,
    p1_ss, p1_rs, ssq_ss, ssq_rs, h_ss, h_rs, pr_ss, pr_rs,
    rz_ss, rz_rs, rx_ss, rx_rs, xs_ss, xs_rs, zs_ss, zs_rs, f_ss, f_rs,
):
    z = lax.axis_index("kv_0")
    x = lax.axis_index("kv_1")
    c = lax.axis_index("tp")
    y = lax.axis_index("dp")
    kv = z * NX + x

    def zp(d):
        return lax.rem(z + d, NZ)

    def xp(d):
        return lax.rem(x + d, NX)

    bar = pltpu.get_barrier_semaphore()

    def greet(i, _):
        pl.semaphore_signal(
            bar, inc=1, device_id={"kv_0": zp(i // NX), "kv_1": xp(i % NX)}, device_id_type=MESH
        )
        return 0

    lax.fori_loop(1, NZ * NX, greet, 0)
    for dx in range(NX):
        pl.semaphore_signal(bar, inc=1, device_id={"kv_1": xp(dx), "tp": 1 - c}, device_id_type=MESH)
    for dy in range(1, 4):
        pl.semaphore_signal(bar, inc=1, device_id={"dp": lax.rem(y + dy, 4)}, device_id_type=MESH)

    def local(src, dst, i):
        cp = pltpu.make_async_copy(src, dst, loc_sem.at[i])
        cp.start()
        return cp

    cq = pl.ds(pl.multiple_of(x * 128, 128), 128)
    cv = pl.ds(pl.multiple_of(x * 256, 256), 256)
    ld_tok = local(tokens, tok_in.at[x, c], 8)
    ld_gains = [local(gain_mix_h, gain_mix, 9), local(gain_mlp_h, gain_mlp, 10)]
    ld_w = [
        local(w_query.at[:, cq], wbuf.at[x, :, 0:128], 0),
        local(w_key.at[:, cq], wbuf.at[x, :, 128:256], 1),
        local(w_value.at[:, cv], wbuf.at[x, :, 256:512], 2),
        local(w_gate.at[:, cv], wbuf.at[x, :, 512:768], 3),
    ]
    ld_st = local(state, st, 4)
    ld_mix = local(w_mix, wm.at[x], 5)
    ld_up = local(w_up, wup.at[c], 6)
    ld_dn = local(w_down, wdn.at[c], 7)

    ld_tok.wait()
    pl.semaphore_wait(bar, 38)

    def remote(src, dst, ss, rs, dev):
        cp = pltpu.make_async_remote_copy(
            src_ref=src, dst_ref=dst, send_sem=ss, recv_sem=rs, device_id=dev, device_id_type=MESH
        )
        cp.start()
        return cp

    tok_cp = []
    for dx in (2, 1, 3):
        tok_cp.append(
            remote(tok_in.at[x, c], tok_in.at[x, c], tok_ss.at[dx], tok_rs.at[dx], {"kv_1": xp(dx)})
        )
    tokp_cp = [remote(tok_in.at[x, c], tok_in.at[x, c], tok_ss.at[4], tok_rs.at[4], {"tp": 1 - c})]

    w_cp = {0: [], 1: [], 2: []}
    for dx in (2, 1, 3):
        dev = {"kv_1": xp(dx)}
        dq = pl.ds(pl.multiple_of(xp(dx) * 128, 128), 128)
        w_cp[0].append(remote(w_query.at[:, dq], wbuf.at[x, :, 0:128], w_ss.at[0, dx], w_rs.at[0, dx], dev))
        w_cp[0].append(remote(w_key.at[:, dq], wbuf.at[x, :, 128:256], w_ss.at[1, dx], w_rs.at[1, dx], dev))
    for j, (w, lo) in enumerate(((w_value, 256), (w_gate, 512))):
        for dx in (2, 1, 3):
            dev = {"kv_1": xp(dx)}
            dv = pl.ds(pl.multiple_of(xp(dx) * 256, 256), 256)
            w_cp[j + 1].append(
                remote(w.at[:, dv], wbuf.at[x, :, lo:lo + 256], w_ss.at[2 + j, dx], w_rs.at[2 + j, dx], dev)
            )

    qrows = pl.ds(pl.multiple_of(y * 256, 256), 256)
    mix_cp = []
    for dx in (2, 1, 3):
        mix_cp.append(
            remote(w_mix.at[qrows], wm.at[x, qrows], mix_ss.at[dx], mix_rs.at[dx], {"kv_1": xp(dx)})
        )

    partner = {"tp": 1 - c}
    mlp_cp = [
        remote(w_up, wup.at[c], mlp_ss.at[0], mlp_rs.at[0], partner),
        remote(w_down, wdn.at[c], mlp_ss.at[1], mlp_rs.at[1], partner),
    ]

    for i, dx in enumerate((1, 3, 2)):
        tok_cp[(1, 2, 0)[i]].wait_recv()
        src = tok_in.at[xp(NX - dx), c]
        tokp_cp.append(remote(src, src, tok_ss.at[4 + dx], tok_rs.at[4 + dx], {"tp": 1 - c}))
    for cp in tokp_cp:
        cp.wait_recv()
    squares = jnp.zeros((256, 128), F32)
    for xx in range(NX):
        both = jnp.transpose(tok_in[xx].reshape(128, 256).astype(F32))
        tokf[:, :, xx * 128:(xx + 1) * 128] = both.reshape(32, 8, 128)
        squares = squares + both * both
    ssq_s[...] = jnp.broadcast_to(jnp.sum(squares, axis=1, keepdims=True), (256, 128)).reshape(32, 8, 128)
    ssq_cp = []
    for dz in FAR:
        ssq_cp.append(
            remote(ssq_s.at[zp(dz) * NX + x], ssq_r.at[dz], ssq_ss.at[dz], ssq_rs.at[dz], {"kv_0": zp(dz)})
        )
    fz = pl.ds(pl.multiple_of(z * 512, 512), 512)
    for ld in ld_gains:
        ld.wait()
    normed = (tokf[...].reshape(256, 512) * gain_mix[:, fz]).astype(BF16)

    for ch in range(3):
        for cp in w_cp[ch]:
            cp.wait_recv()
        for ld in (ld_w[0:2], ld_w[2:3], ld_w[3:4])[ch]:
            ld.wait()
        wch = wbuf[:, :, ch * 256:(ch + 1) * 256].reshape(512, 256)
        part = jnp.dot(normed, wch, preferred_element_type=F32).reshape(32, 8, 256)
        sbuf[ch] = jnp.concatenate([part[:, :, :128], part[:, :, 128:]], axis=1).astype(BF16)

        def scatter(i, _, ch=ch):
            zz, xx = zp(i // NX), xp(i % NX)
            remote(
                sbuf.at[ch, zz * NX + xx], rbuf.at[ch, i], p1_ss.at[ch], p1_rs.at[ch], {"kv_0": zz, "kv_1": xx}
            )
            return 0

        lax.fori_loop(1, NZ * NX, scatter, 0)

    my_cp = []
    for i, dx in enumerate((2, 1, 3)):
        mix_cp[i].wait_recv()
        src = wm.at[xp(NX - dx), qrows]
        for dy in (2, 1, 3):
            my_cp.append(remote(src, src, my_ss.at[dx, dy], my_rs.at[dx, dy], {"dp": lax.rem(y + dy, 4)}))

    for cp in ssq_cp:
        cp.wait_recv()
    ssq_r[0] = ssq_s[kv]
    total = jnp.sum(ssq_r[...], axis=0)
    first_scale = lax.rsqrt(total / 4096.0 + EPS)
    scale16 = jnp.concatenate([first_scale, first_scale], axis=0)[None]

    def own(ch):
        pltpu.make_async_copy(rbuf.at[ch, 1:32], rbuf.at[ch, 1:32], p1_rs.at[ch]).wait()
        rbuf[ch, 0] = sbuf[ch, kv]
        summed = jnp.sum(rbuf[ch].astype(F32).reshape(NZ, NX, 16, 128), axis=0)
        return (summed * scale16).astype(BF16).astype(F32)

    qk = own(0)
    for dx in range(NX):
        qk_abs[xp(NX - dx)] = qk[dx]
    vals = own(1)
    for dx in range(NX):
        v_abs[xp(NX - dx)] = vals[dx]
    qs = qk_abs[:, :8].reshape(32, 128)
    ks = qk_abs[:, 8:].reshape(32, 128) * 0.125
    turned = jnp.transpose(jnp.concatenate([qs, ks, jnp.zeros((64, 128), F32)], axis=0))
    keys_out[...] = turned
    vals_out[...] = v_abs[...]
    ld_st.wait()
    decays = [jnp.exp(-jnp.full((1, 128), rates[c * 8 + h], F32)) for h in range(8)]
    for xs in range(NX):
        for b in range(8):
            for hh in range(2):
                rows = slice(hh * 64, (hh + 1) * 64)
                col = xs * 8 + b
                new = decays[xs * 2 + hh] * st[b, xs, rows, :] + (
                    turned[rows, 32 + col:33 + col] * v_abs[xs, hh * 8 + b:hh * 8 + b + 1, :]
                )
                rdbuf[xs, hh * 8 + b:hh * 8 + b + 1, :] = jnp.sum(
                    turned[rows, col:col + 1] * new, axis=0, keepdims=True
                )
    gates = own(2)
    for dx in range(NX):
        g_abs[xp(NX - dx)] = gates[dx]
    gates = g_abs[...]
    read = rdbuf[...]
    read = read * lax.rsqrt(jnp.mean(read * read, axis=2, keepdims=True) + EPS)
    hall[z] = (gates / (1.0 + jnp.exp(-gates)) * read).astype(BF16)
    h_cp = []
    for dz in FAR:
        h_cp.append(remote(hall.at[z], hall.at[z], h_ss.at[dz], h_rs.at[dz], {"kv_0": zp(dz)}))
    for cp in h_cp:
        cp.wait_recv()
    for cp in my_cp:
        cp.wait_recv()
    ld_mix.wait()

    pieces = []
    for xs in range(NX):
        both = hall[:, xs].astype(F32)
        for hh in range(2):
            pieces.append(both[:, hh * 8:(hh + 1) * 8].reshape(64, 128).astype(BF16))
    lhs = jnp.concatenate(pieces, axis=1)
    for xx in range(NX):
        prod = jnp.dot(lhs, wm[xx], preferred_element_type=F32).astype(BF16)
        pbuf[0, :, xx * 128:(xx + 1) * 128] = prod[:32]
        pbuf[1, :, xx * 128:(xx + 1) * 128] = prod[32:]
    pr_cp = remote(pbuf.at[1 - c], pin, pr_ss, pr_rs, partner)
    pr_cp.wait_recv()
    mixed = pbuf[c].astype(F32) + pin[...].astype(F32)
    own_tok = []
    for zl in range(4):
        own_tok.append(tokf[(c * 4 + zl) * NX + x])
    rg[x, z] = (jnp.concatenate(own_tok, axis=0) + mixed).astype(BF16)

    rz_cp = {}
    for dz in (1, 7, 2, 6, 3, 5, 4):
        rz_cp[dz] = remote(rg.at[x, z], rg.at[x, z], rz_ss.at[dz], rz_rs.at[dz], {"kv_0": zp(dz)})
    rx_cp = []
    ORDER = (0, 1, 7, 2, 6, 3, 5, 4)
    for dz in ORDER:
        zz = lax.rem(z - dz + NZ, NZ)
        if dz:
            rz_cp[dz].wait_recv()
        for dx in (2, 1, 3):
            rx_cp.append(
                remote(rg.at[x, zz], rg.at[x, zz], rx_ss.at[dz, dx], rx_rs.at[dz, dx], {"kv_1": xp(dx)})
            )
    ld_up.wait()
    mlp_cp[0].wait_recv()
    acc = [jnp.zeros((128, 256), F32), jnp.zeros((128, 256), F32)]
    squares = jnp.zeros((128, 128), F32)
    for i, dz in enumerate(ORDER):
        zz = lax.rem(z - dz + NZ, NZ)
        for k in range(3):
            rx_cp[i * 3 + k].wait_recv()
        rows = rg[:, zz].reshape(128, 512).astype(F32)
        fk = pl.ds(pl.multiple_of(zz * 512, 512), 512)
        for q in range(4):
            piece = rows[:, q * 128:(q + 1) * 128]
            squares = squares + piece * piece
        lhs = (rows * gain_mlp[:, fk]).astype(BF16)
        for cc in range(2):
            acc[cc] = acc[cc] + jnp.dot(lhs, wup[cc, fk, :], preferred_element_type=F32)
    second_scale = lax.rsqrt(jnp.sum(squares, axis=1, keepdims=True) / 4096.0 + EPS)
    hid = []
    for cc in range(2):
        upper = jnp.maximum(acc[cc] * second_scale, 0.0)
        hid.append((upper * upper).astype(BF16))

    ld_dn.wait()
    mlp_cp[1].wait_recv()
    xs_cp = {}
    for i in range(NZ):
        dz = (FAR + (0,))[i]
        zz = zp(dz)
        fk = pl.ds(pl.multiple_of(zz * 512, 512), 512)
        part = jnp.dot(hid[0], wdn[0, :, fk], preferred_element_type=F32)
        part = part + jnp.dot(hid[1], wdn[1, :, fk], preferred_element_type=F32)
        part = part.astype(BF16)
        for xx in range(NX):
            xsb[dz, xx] = part[:, xx * 128:(xx + 1) * 128]
        for dx in (2, 1, 3):
            xs_cp[dz, dx] = remote(
                xsb.at[dz, xp(dx)], xrb.at[dz, dx - 1], xs_ss.at[dz, dx], xs_rs.at[dz, dx], {"kv_1": xp(dx)}
            )
    zs_cp = {}
    own_sum = None
    for i in range(NZ):
        dz = (FAR + (0,))[i]
        for dx in (2, 1, 3):
            xs_cp[dz, dx].wait_recv()
        summed = xsb[dz, x].astype(F32) + jnp.sum(xrb[dz].astype(F32), axis=0)
        if dz:
            zsb[dz] = summed.astype(BF16)
            zs_cp[dz] = remote(zsb.at[dz], zrb.at[dz - 1], zs_ss.at[dz], zs_rs.at[dz], {"kv_0": zp(dz)})
        else:
            own_sum = summed
    for dz in FAR:
        zs_cp[dz].wait_recv()
    down = own_sum + jnp.sum(zrb[...].astype(F32), axis=0)
    lanes = pl.ds(pl.multiple_of(x * 128, 128), 128)
    res = rg[:, z, :, lanes].reshape(128, 128).astype(F32)
    fsend[...] = (res + down).astype(BF16)
    f_cp = remote(fsend, frecv, f_ss, f_rs, partner)
    f_cp.wait_recv()
    for who, ref in ((c, fsend), (1 - c, frecv)):
        block = ref[...].astype(F32)
        for xs in range(NX):
            for zl in range(4):
                r0 = xs * 32 + zl * 8
                fin[(who * 4 + zl) * NX + xs] = block[r0:r0 + 8]
    fint[...] = jnp.transpose(fin[...].reshape(256, 128))
    out[...] = fint[pl.ds(pl.multiple_of(c * 64, 64), 64), :].astype(BF16)

    for cp in tok_cp + tokp_cp + w_cp[0] + w_cp[1] + w_cp[2] + mlp_cp + ssq_cp + mix_cp + my_cp + h_cp + [pr_cp]:
        cp.wait_send()
    for ch in range(3):
        pltpu.make_async_copy(sbuf.at[ch, 1:32], sbuf.at[ch, 1:32], p1_ss.at[ch]).wait()
    for cp in list(rz_cp.values()) + rx_cp + list(xs_cp.values()) + list(zs_cp.values()) + [f_cp]:
        cp.wait_send()


def tail(rates, keys_h, vals_h, res_in, state, result, new_state, st, keys, vals, res, ld_sem, out_sem):
    c = lax.axis_index("tp")

    def load(src, dst, i):
        cp = pltpu.make_async_copy(src, dst, ld_sem.at[i])
        cp.start()
        return cp

    small = [load(keys_h, keys, 8), load(vals_h, vals, 9)]
    loads = [load(state.at[b], st.at[b], b) for b in range(8)]
    res_cp = load(res_in, res, 10)
    decays = [jnp.exp(-jnp.full((1, 128), rates[c * 8 + h], F32)) for h in range(8)]
    for cp in small:
        cp.wait()
    stores = []
    for b in range(8):
        loads[b].wait()
        for xs in range(NX):
            for hh in range(2):
                rows = slice(hh * 64, (hh + 1) * 64)
                col = 32 + xs * 8 + b
                st[b, xs, rows, :] = decays[xs * 2 + hh] * st[b, xs, rows, :] + (
                    keys[rows, col:col + 1] * vals[xs, hh * 8 + b:hh * 8 + b + 1, :]
                )
        stores.append(pltpu.make_async_copy(st.at[b], new_state.at[b], out_sem.at[b]))
        stores[-1].start()
        if b == 0:
            res_cp.wait()
            stores.append(pltpu.make_async_copy(res, result, out_sem.at[8]))
            stores[-1].start()
    for cp in stores:
        cp.wait()


def per_device(
    tokens, gain_mix, gain_mlp, decay_rate, w_query, w_key, w_value, w_gate, w_mix, w_up, w_down, state
):
    vm = pl.BlockSpec(memory_space=pltpu.VMEM)
    sm = pl.BlockSpec(memory_space=pltpu.SMEM)
    hbm = pl.BlockSpec(memory_space=pltpu.HBM)
    dma = pltpu.SemaphoreType.DMA
    state = state.reshape(8, 4, 128, 128)
    result, keys, vals = pl.pallas_call(
        kernel,
        out_shape=(
            jax.ShapeDtypeStruct((64, 256), BF16),
            jax.ShapeDtypeStruct((128, 128), F32),
            jax.ShapeDtypeStruct((4, 16, 128), F32),
        ),
        in_specs=[hbm, hbm, hbm, sm] + [hbm] * 8,
        out_specs=(vm, vm, vm),
        scratch_shapes=[
            pltpu.VMEM((1, 4096), F32),
            pltpu.VMEM((1, 4096), F32),
            pltpu.VMEM((4, 2, 64, 256), BF16),
            pltpu.VMEM((32, 8, 512), F32),
            pltpu.VMEM((4, 128, 768), BF16),
            pltpu.VMEM((4, 1024, 128), BF16),
            pltpu.VMEM((2, 4096, 256), BF16),
            pltpu.VMEM((2, 256, 4096), BF16),
            pltpu.VMEM((8, 4, 128, 128), F32),
            pltpu.VMEM((3, 32, 16, 128), BF16),
            pltpu.VMEM((3, 32, 16, 128), BF16),
            pltpu.VMEM((32, 8, 128), F32),
            pltpu.VMEM((8, 8, 128), F32),
            pltpu.VMEM((4, 16, 128), F32),
            pltpu.VMEM((4, 16, 128), F32),
            pltpu.VMEM((4, 16, 128), F32),
            pltpu.VMEM((4, 16, 128), F32),
            pltpu.VMEM((8, 4, 16, 128), BF16),
            pltpu.VMEM((2, 32, 512), BF16),
            pltpu.VMEM((32, 512), BF16),
            pltpu.VMEM((4, 8, 32, 512), BF16),
            pltpu.VMEM((8, 4, 128, 128), BF16),
            pltpu.VMEM((8, 3, 128, 128), BF16),
            pltpu.VMEM((8, 128, 128), BF16),
            pltpu.VMEM((7, 128, 128), BF16),
            pltpu.VMEM((128, 128), BF16),
            pltpu.VMEM((128, 128), BF16),
            pltpu.VMEM((32, 8, 128), F32),
            pltpu.VMEM((128, 256), F32),
            dma((11,)), dma((8,)), dma((8,)), dma((4, 4)), dma((4, 4)), dma((4,)), dma((4,)), dma((4, 4)), dma((4, 4)),
            dma((2,)), dma((2,)), dma((3,)), dma((3,)), dma((8,)), dma((8,)), dma((8,)), dma((8,)),
            dma, dma, dma((8,)), dma((8,)), dma((8, 4)), dma((8, 4)), dma((8, 4)), dma((8, 4)),
            dma((8,)), dma((8,)), dma, dma,
        ],
        compiler_params=pltpu.CompilerParams(
            collective_id=0, has_side_effects=True, vmem_limit_bytes=60 * 1024 * 1024
        ),
        name="layer",
    )(
        tokens.T, gain_mix.reshape(1, 4096), gain_mlp.reshape(1, 4096), decay_rate,
        w_query, w_key, w_value, w_gate, w_mix, w_up, w_down, state,
    )
    result, new_state = pl.pallas_call(
        tail,
        out_shape=(
            jax.ShapeDtypeStruct((64, 256), BF16),
            jax.ShapeDtypeStruct((8, 4, 128, 128), F32),
        ),
        in_specs=[sm, hbm, hbm, hbm, hbm],
        out_specs=(hbm, hbm),
        scratch_shapes=[
            pltpu.VMEM((8, 4, 128, 128), F32),
            pltpu.VMEM((128, 128), F32),
            pltpu.VMEM((4, 16, 128), F32),
            pltpu.VMEM((64, 256), BF16),
            dma((11,)), dma((9,)),
        ],
        compiler_params=pltpu.CompilerParams(vmem_limit_bytes=60 * 1024 * 1024),
        name="tail",
    )(decay_rate, keys, vals, result, state)
    return result.T, new_state.reshape(8, 8, 64, 128)


def solution(mesh):
    torus = Mesh(
        mesh.devices.reshape(mesh.shape["dp"], 8, 4, mesh.shape["tp"]), ("dp", "kv_0", "kv_1", "tp")
    )
    return jax.shard_map(
        per_device,
        mesh=torus,
        in_specs=(
            P("dp", KV_TP),
            P(),
            P(),
            P(),
            P(KV, "tp"),
            P(KV, "tp"),
            P(KV, "tp"),
            P(KV, "tp"),
            P("tp", KV),
            P(None, KV_TP),
            P(KV_TP, None),
            P(DP_KV, "tp", None, None),
        ),
        out_specs=(P("dp", KV_TP), P(DP_KV, "tp", None, None)),
        check_vma=False,
    )
```

```python
import jax
import jax.numpy as jnp
from jax import lax
from jax.sharding import Mesh
from jax.sharding import PartitionSpec as P
from jax.experimental import pallas as pl
from jax.experimental.pallas import tpu as pltpu

KV = ("kv_0", "kv_1")
KV_TP = ("kv_0", "kv_1", "tp")
DP_KV = ("dp", "kv_0", "kv_1")
EPS = 1e-06
F32 = jnp.float32
BF16 = jnp.bfloat16
MESH = pl.DeviceIdType.MESH
NZ = 8
NX = 4
FAR = (4, 3, 5, 2, 6, 1, 7)


def kernel(
    tokens, gain_mix_h, gain_mlp_h, rates, w_query, w_key, w_value, w_gate, w_mix, w_up, w_down, state,
    out, keys_out, vals_out,
    gain_mix, gain_mlp, tok_in, tokf, wbuf, wm, wup, wdn, st,
    sbuf, rbuf, ssq_s, ssq_r, qk_abs, v_abs, g_abs, rdbuf, hall, pbuf, pin, rg,
    xsb, xrb, zsb, zrb, bzs, bzr, bxs, bxr, fsend, frecv, fin, fint,
    loc_sem, tok_ss, tok_rs, w_ss, w_rs, mix_ss, mix_rs, my_ss, my_rs, mlp_ss, mlp_rs,
    p1_ss, p1_rs, ssq_ss, ssq_rs, h_ss, h_rs, pr_ss, pr_rs,
    rz_ss, rz_rs, rx_ss, rx_rs, xs_ss, xs_rs, zs_ss, zs_rs, bz_ss, bz_rs, bx_ss, bx_rs, f_ss, f_rs,
):
    z = lax.axis_index("kv_0")
    x = lax.axis_index("kv_1")
    c = lax.axis_index("tp")
    y = lax.axis_index("dp")
    kv = z * NX + x

    def zp(d):
        return lax.rem(z + d, NZ)

    def xp(d):
        return lax.rem(x + d, NX)

    bar = pltpu.get_barrier_semaphore()

    def greet(i, _):
        pl.semaphore_signal(
            bar, inc=1, device_id={"kv_0": zp(i // NX), "kv_1": xp(i % NX)}, device_id_type=MESH
        )
        return 0

    lax.fori_loop(1, NZ * NX, greet, 0)
    for dx in range(NX):
        pl.semaphore_signal(bar, inc=1, device_id={"kv_1": xp(dx), "tp": 1 - c}, device_id_type=MESH)
    for dy in range(1, 4):
        pl.semaphore_signal(bar, inc=1, device_id={"dp": lax.rem(y + dy, 4)}, device_id_type=MESH)

    def local(src, dst, i):
        cp = pltpu.make_async_copy(src, dst, loc_sem.at[i])
        cp.start()
        return cp

    cq = pl.ds(pl.multiple_of(x * 128, 128), 128)
    cv = pl.ds(pl.multiple_of(x * 256, 256), 256)
    ld_tok = local(tokens, tok_in.at[x, c], 8)
    ld_gains = [local(gain_mix_h, gain_mix, 9), local(gain_mlp_h, gain_mlp, 10)]
    ld_w = [
        local(w_query.at[:, cq], wbuf.at[x, :, 0:128], 0),
        local(w_key.at[:, cq], wbuf.at[x, :, 128:256], 1),
        local(w_value.at[:, cv], wbuf.at[x, :, 256:512], 2),
        local(w_gate.at[:, cv], wbuf.at[x, :, 512:768], 3),
    ]
    ld_st = local(state, st, 4)
    ld_mix = local(w_mix, wm.at[x], 5)
    ld_up = local(w_up, wup.at[c], 6)
    ld_dn = local(w_down, wdn.at[c], 7)

    ld_tok.wait()
    pl.semaphore_wait(bar, 38)

    def remote(src, dst, ss, rs, dev):
        cp = pltpu.make_async_remote_copy(
            src_ref=src, dst_ref=dst, send_sem=ss, recv_sem=rs, device_id=dev, device_id_type=MESH
        )
        cp.start()
        return cp

    tok_cp = []
    for dx in (2, 1, 3):
        tok_cp.append(
            remote(tok_in.at[x, c], tok_in.at[x, c], tok_ss.at[dx], tok_rs.at[dx], {"kv_1": xp(dx)})
        )
    tokp_cp = [remote(tok_in.at[x, c], tok_in.at[x, c], tok_ss.at[4], tok_rs.at[4], {"tp": 1 - c})]

    w_cp = {0: [], 1: [], 2: []}
    for dx in (2, 1, 3):
        dev = {"kv_1": xp(dx)}
        dq = pl.ds(pl.multiple_of(xp(dx) * 128, 128), 128)
        w_cp[0].append(remote(w_query.at[:, dq], wbuf.at[x, :, 0:128], w_ss.at[0, dx], w_rs.at[0, dx], dev))
        w_cp[0].append(remote(w_key.at[:, dq], wbuf.at[x, :, 128:256], w_ss.at[1, dx], w_rs.at[1, dx], dev))
    for j, (w, lo) in enumerate(((w_value, 256), (w_gate, 512))):
        for dx in (2, 1, 3):
            dev = {"kv_1": xp(dx)}
            dv = pl.ds(pl.multiple_of(xp(dx) * 256, 256), 256)
            w_cp[j + 1].append(
                remote(w.at[:, dv], wbuf.at[x, :, lo:lo + 256], w_ss.at[2 + j, dx], w_rs.at[2 + j, dx], dev)
            )

    qrows = pl.ds(pl.multiple_of(y * 256, 256), 256)
    mix_cp = []
    for dx in (2, 1, 3):
        mix_cp.append(
            remote(w_mix.at[qrows], wm.at[x, qrows], mix_ss.at[dx], mix_rs.at[dx], {"kv_1": xp(dx)})
        )

    partner = {"tp": 1 - c}
    mlp_cp = [
        remote(w_up, wup.at[c], mlp_ss.at[0], mlp_rs.at[0], partner),
        remote(w_down, wdn.at[c], mlp_ss.at[1], mlp_rs.at[1], partner),
    ]

    for i, dx in enumerate((1, 3, 2)):
        tok_cp[(1, 2, 0)[i]].wait_recv()
        src = tok_in.at[xp(NX - dx), c]
        tokp_cp.append(remote(src, src, tok_ss.at[4 + dx], tok_rs.at[4 + dx], {"tp": 1 - c}))
    for cp in tokp_cp:
        cp.wait_recv()
    squares = jnp.zeros((256, 128), F32)
    for xx in range(NX):
        both = jnp.transpose(tok_in[xx].reshape(128, 256).astype(F32))
        tokf[:, :, xx * 128:(xx + 1) * 128] = both.reshape(32, 8, 128)
        squares = squares + both * both
    ssq_s[...] = jnp.broadcast_to(jnp.sum(squares, axis=1, keepdims=True), (256, 128)).reshape(32, 8, 128)
    ssq_cp = []
    for dz in FAR:
        ssq_cp.append(
            remote(ssq_s.at[zp(dz) * NX + x], ssq_r.at[dz], ssq_ss.at[dz], ssq_rs.at[dz], {"kv_0": zp(dz)})
        )
    fz = pl.ds(pl.multiple_of(z * 512, 512), 512)
    for ld in ld_gains:
        ld.wait()
    normed = (tokf[...].reshape(256, 512) * gain_mix[:, fz]).astype(BF16)

    for ch in range(3):
        for cp in w_cp[ch]:
            cp.wait_recv()
        for ld in (ld_w[0:2], ld_w[2:3], ld_w[3:4])[ch]:
            ld.wait()
        wch = wbuf[:, :, ch * 256:(ch + 1) * 256].reshape(512, 256)
        part = jnp.dot(normed, wch, preferred_element_type=F32).reshape(32, 8, 256)
        sbuf[ch] = jnp.concatenate([part[:, :, :128], part[:, :, 128:]], axis=1).astype(BF16)

        def scatter(i, _, ch=ch):
            zz, xx = zp(i // NX), xp(i % NX)
            remote(
                sbuf.at[ch, zz * NX + xx], rbuf.at[ch, i], p1_ss.at[ch], p1_rs.at[ch], {"kv_0": zz, "kv_1": xx}
            )
            return 0

        lax.fori_loop(1, NZ * NX, scatter, 0)

    my_cp = []
    for i, dx in enumerate((2, 1, 3)):
        mix_cp[i].wait_recv()
        src = wm.at[xp(NX - dx), qrows]
        for dy in (2, 1, 3):
            my_cp.append(remote(src, src, my_ss.at[dx, dy], my_rs.at[dx, dy], {"dp": lax.rem(y + dy, 4)}))

    for cp in ssq_cp:
        cp.wait_recv()
    ssq_r[0] = ssq_s[kv]
    total = jnp.sum(ssq_r[...], axis=0)
    first_scale = lax.rsqrt(total / 4096.0 + EPS)
    scale16 = jnp.concatenate([first_scale, first_scale], axis=0)[None]

    def own(ch):
        pltpu.make_async_copy(rbuf.at[ch, 1:32], rbuf.at[ch, 1:32], p1_rs.at[ch]).wait()
        rbuf[ch, 0] = sbuf[ch, kv]
        summed = jnp.sum(rbuf[ch].astype(F32).reshape(NZ, NX, 16, 128), axis=0)
        return (summed * scale16).astype(BF16).astype(F32)

    qk = own(0)
    for dx in range(NX):
        qk_abs[xp(NX - dx)] = qk[dx]
    vals = own(1)
    for dx in range(NX):
        v_abs[xp(NX - dx)] = vals[dx]
    qs = qk_abs[:, :8].reshape(32, 128)
    ks = qk_abs[:, 8:].reshape(32, 128) * 0.125
    turned = jnp.transpose(jnp.concatenate([qs, ks, jnp.zeros((64, 128), F32)], axis=0))
    keys_out[...] = turned
    vals_out[...] = v_abs[...]
    ld_st.wait()
    decays = [jnp.exp(-jnp.full((1, 128), rates[c * 8 + h], F32)) for h in range(8)]
    for xs in range(NX):
        for b in range(8):
            for hh in range(2):
                rows = slice(hh * 64, (hh + 1) * 64)
                col = xs * 8 + b
                new = decays[xs * 2 + hh] * st[b, xs, rows, :] + (
                    turned[rows, 32 + col:33 + col] * v_abs[xs, hh * 8 + b:hh * 8 + b + 1, :]
                )
                rdbuf[xs, hh * 8 + b:hh * 8 + b + 1, :] = jnp.sum(
                    turned[rows, col:col + 1] * new, axis=0, keepdims=True
                )
    gates = own(2)
    for dx in range(NX):
        g_abs[xp(NX - dx)] = gates[dx]
    gates = g_abs[...]
    read = rdbuf[...]
    read = read * lax.rsqrt(jnp.mean(read * read, axis=2, keepdims=True) + EPS)
    hall[z] = (gates / (1.0 + jnp.exp(-gates)) * read).astype(BF16)
    h_cp = []
    for dz in FAR:
        h_cp.append(remote(hall.at[z], hall.at[z], h_ss.at[dz], h_rs.at[dz], {"kv_0": zp(dz)}))
    for cp in h_cp:
        cp.wait_recv()
    for cp in my_cp:
        cp.wait_recv()
    ld_mix.wait()

    pieces = []
    for xs in range(NX):
        both = hall[:, xs].astype(F32)
        for hh in range(2):
            pieces.append(both[:, hh * 8:(hh + 1) * 8].reshape(64, 128).astype(BF16))
    lhs = jnp.concatenate(pieces, axis=1)
    for xx in range(NX):
        prod = jnp.dot(lhs, wm[xx], preferred_element_type=F32).astype(BF16)
        pbuf[0, :, xx * 128:(xx + 1) * 128] = prod[:32]
        pbuf[1, :, xx * 128:(xx + 1) * 128] = prod[32:]
    pr_cp = remote(pbuf.at[1 - c], pin, pr_ss, pr_rs, partner)
    pr_cp.wait_recv()
    mixed = pbuf[c].astype(F32) + pin[...].astype(F32)
    own_tok = []
    for zl in range(4):
        own_tok.append(tokf[(c * 4 + zl) * NX + x])
    rg[x, z] = (jnp.concatenate(own_tok, axis=0) + mixed).astype(BF16)

    rz_cp = {}
    for dz in (1, 7, 2, 6, 3, 5, 4):
        rz_cp[dz] = remote(rg.at[x, z], rg.at[x, z], rz_ss.at[dz], rz_rs.at[dz], {"kv_0": zp(dz)})
    rx_cp = []
    ORDER = (0, 1, 7, 2, 6, 3, 5, 4)
    for dz in ORDER:
        zz = lax.rem(z - dz + NZ, NZ)
        if dz:
            rz_cp[dz].wait_recv()
        for dx in (2, 1, 3):
            rx_cp.append(
                remote(rg.at[x, zz], rg.at[x, zz], rx_ss.at[dz, dx], rx_rs.at[dz, dx], {"kv_1": xp(dx)})
            )
    ld_up.wait()
    mlp_cp[0].wait_recv()
    acc = [jnp.zeros((128, 256), F32), jnp.zeros((128, 256), F32)]
    squares = jnp.zeros((128, 128), F32)
    for i, dz in enumerate(ORDER):
        zz = lax.rem(z - dz + NZ, NZ)
        for k in range(3):
            rx_cp[i * 3 + k].wait_recv()
        rows = rg[:, zz].reshape(128, 512).astype(F32)
        fk = pl.ds(pl.multiple_of(zz * 512, 512), 512)
        for q in range(4):
            piece = rows[:, q * 128:(q + 1) * 128]
            squares = squares + piece * piece
        lhs = (rows * gain_mlp[:, fk]).astype(BF16)
        for cc in range(2):
            acc[cc] = acc[cc] + jnp.dot(lhs, wup[cc, fk, :], preferred_element_type=F32)
    second_scale = lax.rsqrt(jnp.sum(squares, axis=1, keepdims=True) / 4096.0 + EPS)
    hid = []
    for cc in range(2):
        upper = jnp.maximum(acc[cc] * second_scale, 0.0)
        hid.append((upper * upper).astype(BF16))

    ld_dn.wait()
    mlp_cp[1].wait_recv()
    xs_cp = {}
    bz_cp = {}
    for i in range(NZ):
        dz = (FAR + (0,))[i]
        zz = zp(dz)
        fk = pl.ds(pl.multiple_of(zz * 512, 512), 512)
        part = jnp.dot(hid[0], wdn[0, :, fk], preferred_element_type=F32)
        part = part + jnp.dot(hid[1], wdn[1, :, fk], preferred_element_type=F32)
        part = part.astype(BF16)
        for xx in range(NX):
            xsb[dz, xx] = part[:96, xx * 128:(xx + 1) * 128]
            bzs[dz, xx] = part[96:, xx * 128:(xx + 1) * 128]
        if dz:
            bz_cp[dz] = remote(bzs.at[dz], bzr.at[dz - 1], bz_ss.at[dz], bz_rs.at[dz], {"kv_0": zp(dz)})
        for dx in (2, 1, 3):
            xs_cp[dz, dx] = remote(
                xsb.at[dz, xp(dx)], xrb.at[dz, dx - 1], xs_ss.at[dz, dx], xs_rs.at[dz, dx], {"kv_1": xp(dx)}
            )
    zs_cp = {}
    own_sum = None
    for i in range(NZ):
        dz = (FAR + (0,))[i]
        for dx in (2, 1, 3):
            xs_cp[dz, dx].wait_recv()
        summed = xsb[dz, x].astype(F32) + jnp.sum(xrb[dz].astype(F32), axis=0)
        if dz:
            zsb[dz] = summed.astype(BF16)
            zs_cp[dz] = remote(zsb.at[dz], zrb.at[dz - 1], zs_ss.at[dz], zs_rs.at[dz], {"kv_0": zp(dz)})
        else:
            own_sum = summed
    for dz in FAR:
        bz_cp[dz].wait_recv()
    last = bzs[0].astype(F32) + jnp.sum(bzr[...].astype(F32), axis=0)
    bxs[...] = last.astype(BF16)
    bx_cp = []
    for dx in (2, 1, 3):
        bx_cp.append(
            remote(bxs.at[xp(dx)], bxr.at[dx - 1], bx_ss.at[dx], bx_rs.at[dx], {"kv_1": xp(dx)})
        )
    for dz in FAR:
        zs_cp[dz].wait_recv()
    first = own_sum + jnp.sum(zrb[...].astype(F32), axis=0)
    for cp in bx_cp:
        cp.wait_recv()
    last = bxs[x].astype(F32) + jnp.sum(bxr[...].astype(F32), axis=0)
    down = jnp.concatenate([first, last], axis=0)
    lanes = pl.ds(pl.multiple_of(x * 128, 128), 128)
    res = rg[:, z, :, lanes].reshape(128, 128).astype(F32)
    fsend[...] = (res + down).astype(BF16)
    f_cp = remote(fsend, frecv, f_ss, f_rs, partner)
    f_cp.wait_recv()
    for who, ref in ((c, fsend), (1 - c, frecv)):
        block = ref[...].astype(F32)
        for xs in range(NX):
            for zl in range(4):
                r0 = xs * 32 + zl * 8
                fin[(who * 4 + zl) * NX + xs] = block[r0:r0 + 8]
    fint[...] = jnp.transpose(fin[...].reshape(256, 128))
    out[...] = fint[pl.ds(pl.multiple_of(c * 64, 64), 64), :].astype(BF16)

    for cp in tok_cp + tokp_cp + w_cp[0] + w_cp[1] + w_cp[2] + mlp_cp + ssq_cp + mix_cp + my_cp + h_cp + [pr_cp]:
        cp.wait_send()
    for ch in range(3):
        pltpu.make_async_copy(sbuf.at[ch, 1:32], sbuf.at[ch, 1:32], p1_ss.at[ch]).wait()
    for cp in list(rz_cp.values()) + rx_cp + list(xs_cp.values()) + list(zs_cp.values()) + list(bz_cp.values()) + bx_cp + [f_cp]:
        cp.wait_send()


def tail(rates, keys_h, vals_h, res_in, state, result, new_state, st, keys, vals, res, ld_sem, out_sem):
    c = lax.axis_index("tp")

    def load(src, dst, i):
        cp = pltpu.make_async_copy(src, dst, ld_sem.at[i])
        cp.start()
        return cp

    small = [load(keys_h, keys, 8), load(vals_h, vals, 9)]
    loads = [load(state.at[b], st.at[b], b) for b in range(8)]
    res_cp = load(res_in, res, 10)
    decays = [jnp.exp(-jnp.full((1, 128), rates[c * 8 + h], F32)) for h in range(8)]
    for cp in small:
        cp.wait()
    stores = []
    for b in range(8):
        loads[b].wait()
        for xs in range(NX):
            for hh in range(2):
                rows = slice(hh * 64, (hh + 1) * 64)
                col = 32 + xs * 8 + b
                st[b, xs, rows, :] = decays[xs * 2 + hh] * st[b, xs, rows, :] + (
                    keys[rows, col:col + 1] * vals[xs, hh * 8 + b:hh * 8 + b + 1, :]
                )
        stores.append(pltpu.make_async_copy(st.at[b], new_state.at[b], out_sem.at[b]))
        stores[-1].start()
        if b == 0:
            res_cp.wait()
            stores.append(pltpu.make_async_copy(res, result, out_sem.at[8]))
            stores[-1].start()
    for cp in stores:
        cp.wait()


def per_device(
    tokens, gain_mix, gain_mlp, decay_rate, w_query, w_key, w_value, w_gate, w_mix, w_up, w_down, state
):
    vm = pl.BlockSpec(memory_space=pltpu.VMEM)
    sm = pl.BlockSpec(memory_space=pltpu.SMEM)
    hbm = pl.BlockSpec(memory_space=pltpu.HBM)
    dma = pltpu.SemaphoreType.DMA
    state = state.reshape(8, 4, 128, 128)
    result, keys, vals = pl.pallas_call(
        kernel,
        out_shape=(
            jax.ShapeDtypeStruct((64, 256), BF16),
            jax.ShapeDtypeStruct((128, 128), F32),
            jax.ShapeDtypeStruct((4, 16, 128), F32),
        ),
        in_specs=[hbm, hbm, hbm, sm] + [hbm] * 8,
        out_specs=(vm, vm, vm),
        scratch_shapes=[
            pltpu.VMEM((1, 4096), F32),
            pltpu.VMEM((1, 4096), F32),
            pltpu.VMEM((4, 2, 64, 256), BF16),
            pltpu.VMEM((32, 8, 512), F32),
            pltpu.VMEM((4, 128, 768), BF16),
            pltpu.VMEM((4, 1024, 128), BF16),
            pltpu.VMEM((2, 4096, 256), BF16),
            pltpu.VMEM((2, 256, 4096), BF16),
            pltpu.VMEM((8, 4, 128, 128), F32),
            pltpu.VMEM((3, 32, 16, 128), BF16),
            pltpu.VMEM((3, 32, 16, 128), BF16),
            pltpu.VMEM((32, 8, 128), F32),
            pltpu.VMEM((8, 8, 128), F32),
            pltpu.VMEM((4, 16, 128), F32),
            pltpu.VMEM((4, 16, 128), F32),
            pltpu.VMEM((4, 16, 128), F32),
            pltpu.VMEM((4, 16, 128), F32),
            pltpu.VMEM((8, 4, 16, 128), BF16),
            pltpu.VMEM((2, 32, 512), BF16),
            pltpu.VMEM((32, 512), BF16),
            pltpu.VMEM((4, 8, 32, 512), BF16),
            pltpu.VMEM((8, 4, 96, 128), BF16),
            pltpu.VMEM((8, 3, 96, 128), BF16),
            pltpu.VMEM((8, 96, 128), BF16),
            pltpu.VMEM((7, 96, 128), BF16),
            pltpu.VMEM((8, 4, 32, 128), BF16),
            pltpu.VMEM((7, 4, 32, 128), BF16),
            pltpu.VMEM((4, 32, 128), BF16),
            pltpu.VMEM((3, 32, 128), BF16),
            pltpu.VMEM((128, 128), BF16),
            pltpu.VMEM((128, 128), BF16),
            pltpu.VMEM((32, 8, 128), F32),
            pltpu.VMEM((128, 256), F32),
            dma((11,)), dma((8,)), dma((8,)), dma((4, 4)), dma((4, 4)), dma((4,)), dma((4,)), dma((4, 4)), dma((4, 4)),
            dma((2,)), dma((2,)), dma((3,)), dma((3,)), dma((8,)), dma((8,)), dma((8,)), dma((8,)),
            dma, dma, dma((8,)), dma((8,)), dma((8, 4)), dma((8, 4)), dma((8, 4)), dma((8, 4)),
            dma((8,)), dma((8,)), dma((8,)), dma((8,)), dma((4,)), dma((4,)), dma, dma,
        ],
        compiler_params=pltpu.CompilerParams(
            collective_id=0, has_side_effects=True, vmem_limit_bytes=60 * 1024 * 1024
        ),
        name="layer",
    )(
        tokens.T, gain_mix.reshape(1, 4096), gain_mlp.reshape(1, 4096), decay_rate,
        w_query, w_key, w_value, w_gate, w_mix, w_up, w_down, state,
    )
    result, new_state = pl.pallas_call(
        tail,
        out_shape=(
            jax.ShapeDtypeStruct((64, 256), BF16),
            jax.ShapeDtypeStruct((8, 4, 128, 128), F32),
        ),
        in_specs=[sm, hbm, hbm, hbm, hbm],
        out_specs=(hbm, hbm),
        scratch_shapes=[
            pltpu.VMEM((8, 4, 128, 128), F32),
            pltpu.VMEM((128, 128), F32),
            pltpu.VMEM((4, 16, 128), F32),
            pltpu.VMEM((64, 256), BF16),
            dma((11,)), dma((9,)),
        ],
        compiler_params=pltpu.CompilerParams(vmem_limit_bytes=60 * 1024 * 1024),
        name="tail",
    )(decay_rate, keys, vals, result, state)
    return result.T, new_state.reshape(8, 8, 64, 128)


def solution(mesh):
    torus = Mesh(
        mesh.devices.reshape(mesh.shape["dp"], 8, 4, mesh.shape["tp"]), ("dp", "kv_0", "kv_1", "tp")
    )
    return jax.shard_map(
        per_device,
        mesh=torus,
        in_specs=(
            P("dp", KV_TP),
            P(),
            P(),
            P(),
            P(KV, "tp"),
            P(KV, "tp"),
            P(KV, "tp"),
            P(KV, "tp"),
            P("tp", KV),
            P(None, KV_TP),
            P(KV_TP, None),
            P(DP_KV, "tp", None, None),
        ),
        out_specs=(P("dp", KV_TP), P(DP_KV, "tp", None, None)),
        check_vma=False,
    )
```

```python
import jax
import jax.numpy as jnp
from jax import lax
from jax.sharding import Mesh
from jax.sharding import PartitionSpec as P
from jax.experimental import pallas as pl
from jax.experimental.pallas import tpu as pltpu

KV = ("kv_0", "kv_1")
KV_TP = ("kv_0", "kv_1", "tp")
DP_KV = ("dp", "kv_0", "kv_1")
EPS = 1e-06
F32 = jnp.float32
BF16 = jnp.bfloat16
MESH = pl.DeviceIdType.MESH
NZ = 8
NX = 4
FAR = (4, 3, 5, 2, 6, 1, 7)


def kernel(
    tokens, gain_mix_h, gain_mlp_h, rates, w_query, w_key, w_value, w_gate, w_mix, w_up, w_down, state,
    out, new_state,
    gain_mix, gain_mlp, tok_in, tokf, wbuf, wm, wup, wdn, st,
    sbuf, rbuf, ssq_s, ssq_r, qk_abs, v_abs, g_abs, rdbuf, hall, pbuf, pin, rg,
    xsb, xrb, zsb, zrb, bzs, bzr, bxs, bxr, fsend, frecv, fin, fint,
    loc_sem, ns_sem, tok_ss, tok_rs, w_ss, w_rs, mix_ss, mix_rs, my_ss, my_rs, mlp_ss, mlp_rs,
    p1_ss, p1_rs, ssq_ss, ssq_rs, h_ss, h_rs, pr_ss, pr_rs,
    rz_ss, rz_rs, rx_ss, rx_rs, xs_ss, xs_rs, zs_ss, zs_rs, bz_ss, bz_rs, bx_ss, bx_rs, f_ss, f_rs,
):
    z = lax.axis_index("kv_0")
    x = lax.axis_index("kv_1")
    c = lax.axis_index("tp")
    y = lax.axis_index("dp")
    kv = z * NX + x

    def zp(d):
        return lax.rem(z + d, NZ)

    def xp(d):
        return lax.rem(x + d, NX)

    bar = pltpu.get_barrier_semaphore()

    def greet(i, _):
        pl.semaphore_signal(
            bar, inc=1, device_id={"kv_0": zp(i // NX), "kv_1": xp(i % NX)}, device_id_type=MESH
        )
        return 0

    lax.fori_loop(1, NZ * NX, greet, 0)
    pl.semaphore_signal(bar, inc=1, device_id={"tp": 1 - c}, device_id_type=MESH)
    for dy in range(1, 4):
        pl.semaphore_signal(bar, inc=1, device_id={"dp": lax.rem(y + dy, 4)}, device_id_type=MESH)

    def local(src, dst, i):
        cp = pltpu.make_async_copy(src, dst, loc_sem.at[i])
        cp.start()
        return cp

    cq = pl.ds(pl.multiple_of(x * 128, 128), 128)
    cv = pl.ds(pl.multiple_of(x * 256, 256), 256)
    ld_tok = local(tokens, tok_in.at[x, c], 8)
    ld_gains = [local(gain_mix_h, gain_mix, 9), local(gain_mlp_h, gain_mlp, 10)]
    ld_w = [
        local(w_query.at[:, cq], wbuf.at[x, :, 0:128], 0),
        local(w_key.at[:, cq], wbuf.at[x, :, 128:256], 1),
        local(w_value.at[:, cv], wbuf.at[x, :, 256:512], 2),
        local(w_gate.at[:, cv], wbuf.at[x, :, 512:768], 3),
    ]
    ld_st = local(state, st, 4)
    ld_mix = local(w_mix, wm.at[x], 5)
    ld_up = local(w_up, wup.at[c], 6)
    ld_dn = local(w_down, wdn.at[c], 7)

    ld_tok.wait()
    pl.semaphore_wait(bar, 35)

    def remote(src, dst, ss, rs, dev):
        cp = pltpu.make_async_remote_copy(
            src_ref=src, dst_ref=dst, send_sem=ss, recv_sem=rs, device_id=dev, device_id_type=MESH
        )
        cp.start()
        return cp

    tok_cp = []
    for dx in (2, 1, 3):
        tok_cp.append(
            remote(tok_in.at[x, c], tok_in.at[x, c], tok_ss.at[dx], tok_rs.at[dx], {"kv_1": xp(dx)})
        )
    tokp_cp = [remote(tok_in.at[x, c], tok_in.at[x, c], tok_ss.at[4], tok_rs.at[4], {"tp": 1 - c})]

    w_cp = {0: [], 1: [], 2: []}
    for dx in (2, 1, 3):
        dev = {"kv_1": xp(dx)}
        dq = pl.ds(pl.multiple_of(xp(dx) * 128, 128), 128)
        w_cp[0].append(remote(w_query.at[:, dq], wbuf.at[x, :, 0:128], w_ss.at[0, dx], w_rs.at[0, dx], dev))
        w_cp[0].append(remote(w_key.at[:, dq], wbuf.at[x, :, 128:256], w_ss.at[1, dx], w_rs.at[1, dx], dev))
    for j, (w, lo) in enumerate(((w_value, 256), (w_gate, 512))):
        for dx in (2, 1, 3):
            dev = {"kv_1": xp(dx)}
            dv = pl.ds(pl.multiple_of(xp(dx) * 256, 256), 256)
            w_cp[j + 1].append(
                remote(w.at[:, dv], wbuf.at[x, :, lo:lo + 256], w_ss.at[2 + j, dx], w_rs.at[2 + j, dx], dev)
            )

    qrows = pl.ds(pl.multiple_of(y * 256, 256), 256)
    mix_cp = []
    for dx in (2, 1, 3):
        mix_cp.append(
            remote(w_mix.at[qrows], wm.at[x, qrows], mix_ss.at[dx], mix_rs.at[dx], {"kv_1": xp(dx)})
        )

    partner = {"tp": 1 - c}
    mlp_cp = [
        remote(w_up, wup.at[c], mlp_ss.at[0], mlp_rs.at[0], partner),
        remote(w_down, wdn.at[c], mlp_ss.at[1], mlp_rs.at[1], partner),
    ]

    for i, dx in enumerate((1, 3, 2)):
        tok_cp[(1, 2, 0)[i]].wait_recv()
        src = tok_in.at[xp(NX - dx), c]
        tokp_cp.append(remote(src, src, tok_ss.at[4 + dx], tok_rs.at[4 + dx], {"tp": 1 - c}))
    for cp in tokp_cp:
        cp.wait_recv()
    squares = jnp.zeros((256, 128), F32)
    for xx in range(NX):
        both = jnp.transpose(tok_in[xx].reshape(128, 256).astype(F32))
        tokf[:, :, xx * 128:(xx + 1) * 128] = both.reshape(32, 8, 128)
        squares = squares + both * both
    ssq_s[...] = jnp.broadcast_to(jnp.sum(squares, axis=1, keepdims=True), (256, 128)).reshape(32, 8, 128)
    ssq_cp = []
    for dz in FAR:
        ssq_cp.append(
            remote(ssq_s.at[zp(dz) * NX + x], ssq_r.at[dz], ssq_ss.at[dz], ssq_rs.at[dz], {"kv_0": zp(dz)})
        )
    fz = pl.ds(pl.multiple_of(z * 512, 512), 512)
    for ld in ld_gains:
        ld.wait()
    normed = (tokf[...].reshape(256, 512) * gain_mix[:, fz]).astype(BF16)

    for ch in range(3):
        for cp in w_cp[ch]:
            cp.wait_recv()
        for ld in (ld_w[0:2], ld_w[2:3], ld_w[3:4])[ch]:
            ld.wait()
        wch = wbuf[:, :, ch * 256:(ch + 1) * 256].reshape(512, 256)
        part = jnp.dot(normed, wch, preferred_element_type=F32).reshape(32, 8, 256)
        sbuf[ch] = jnp.concatenate([part[:, :, :128], part[:, :, 128:]], axis=1).astype(BF16)

        def scatter(i, _, ch=ch):
            zz, xx = zp(i // NX), xp(i % NX)
            remote(
                sbuf.at[ch, zz * NX + xx], rbuf.at[ch, i], p1_ss.at[ch], p1_rs.at[ch], {"kv_0": zz, "kv_1": xx}
            )
            return 0

        lax.fori_loop(1, NZ * NX, scatter, 0)

    my_cp = []
    for i, dx in enumerate((2, 1, 3)):
        mix_cp[i].wait_recv()
        src = wm.at[xp(NX - dx), qrows]
        for dy in (2, 1, 3):
            my_cp.append(remote(src, src, my_ss.at[dx, dy], my_rs.at[dx, dy], {"dp": lax.rem(y + dy, 4)}))

    for cp in ssq_cp:
        cp.wait_recv()
    ssq_r[0] = ssq_s[kv]
    total = jnp.sum(ssq_r[...], axis=0)
    first_scale = lax.rsqrt(total / 4096.0 + EPS)
    scale16 = jnp.concatenate([first_scale, first_scale], axis=0)[None]

    def own(ch):
        pltpu.make_async_copy(rbuf.at[ch, 1:32], rbuf.at[ch, 1:32], p1_rs.at[ch]).wait()
        rbuf[ch, 0] = sbuf[ch, kv]
        summed = jnp.sum(rbuf[ch].astype(F32).reshape(NZ, NX, 16, 128), axis=0)
        return (summed * scale16).astype(BF16).astype(F32)

    qk = own(0)
    for dx in range(NX):
        qk_abs[xp(NX - dx)] = qk[dx]
    vals = own(1)
    for dx in range(NX):
        v_abs[xp(NX - dx)] = vals[dx]
    qs = qk_abs[:, :8].reshape(32, 128)
    ks = qk_abs[:, 8:].reshape(32, 128) * 0.125
    turned = jnp.transpose(jnp.concatenate([qs, ks, jnp.zeros((64, 128), F32)], axis=0))
    ld_st.wait()
    decays = [jnp.exp(-jnp.full((1, 128), rates[c * 8 + h], F32)) for h in range(8)]
    for xs in range(NX):
        for b in range(8):
            for hh in range(2):
                rows = slice(hh * 64, (hh + 1) * 64)
                col = xs * 8 + b
                new = decays[xs * 2 + hh] * st[b, xs, rows, :] + (
                    turned[rows, 32 + col:33 + col] * v_abs[xs, hh * 8 + b:hh * 8 + b + 1, :]
                )
                st[b, xs, rows, :] = new
                rdbuf[xs, hh * 8 + b:hh * 8 + b + 1, :] = jnp.sum(
                    turned[rows, col:col + 1] * new, axis=0, keepdims=True
                )
    ns_cp = []
    for q in range(4):
        cp = pltpu.make_async_copy(st.at[2 * q:2 * q + 2], new_state.at[2 * q:2 * q + 2], ns_sem.at[q])
        cp.start()
        ns_cp.append(cp)
    gates = own(2)
    for dx in range(NX):
        g_abs[xp(NX - dx)] = gates[dx]
    gates = g_abs[...]
    read = rdbuf[...]
    read = read * lax.rsqrt(jnp.mean(read * read, axis=2, keepdims=True) + EPS)
    hall[z] = (gates / (1.0 + jnp.exp(-gates)) * read).astype(BF16)
    h_cp = []
    for dz in FAR:
        h_cp.append(remote(hall.at[z], hall.at[z], h_ss.at[dz], h_rs.at[dz], {"kv_0": zp(dz)}))
    for cp in h_cp:
        cp.wait_recv()
    for cp in my_cp:
        cp.wait_recv()
    ld_mix.wait()

    pieces = []
    for xs in range(NX):
        both = hall[:, xs].astype(F32)
        for hh in range(2):
            pieces.append(both[:, hh * 8:(hh + 1) * 8].reshape(64, 128).astype(BF16))
    lhs = jnp.concatenate(pieces, axis=1)
    for xx in range(NX):
        prod = jnp.dot(lhs, wm[xx], preferred_element_type=F32).astype(BF16)
        pbuf[0, :, xx * 128:(xx + 1) * 128] = prod[:32]
        pbuf[1, :, xx * 128:(xx + 1) * 128] = prod[32:]
    pr_cp = remote(pbuf.at[1 - c], pin, pr_ss, pr_rs, partner)
    pr_cp.wait_recv()
    mixed = pbuf[c].astype(F32) + pin[...].astype(F32)
    own_tok = []
    for zl in range(4):
        own_tok.append(tokf[(c * 4 + zl) * NX + x])
    rg[x, z] = (jnp.concatenate(own_tok, axis=0) + mixed).astype(BF16)

    rz_cp = {}
    for dz in (1, 7, 2, 6, 3, 5, 4):
        rz_cp[dz] = remote(rg.at[x, z], rg.at[x, z], rz_ss.at[dz], rz_rs.at[dz], {"kv_0": zp(dz)})
    rx_cp = []
    ORDER = (0, 1, 7, 2, 6, 3, 5, 4)
    for dz in ORDER:
        zz = lax.rem(z - dz + NZ, NZ)
        if dz:
            rz_cp[dz].wait_recv()
        for dx in (2, 1, 3):
            rx_cp.append(
                remote(rg.at[x, zz], rg.at[x, zz], rx_ss.at[dz, dx], rx_rs.at[dz, dx], {"kv_1": xp(dx)})
            )
    ld_up.wait()
    mlp_cp[0].wait_recv()
    acc = [jnp.zeros((128, 256), F32), jnp.zeros((128, 256), F32)]
    squares = jnp.zeros((128, 128), F32)
    for i, dz in enumerate(ORDER):
        zz = lax.rem(z - dz + NZ, NZ)
        for k in range(3):
            rx_cp[i * 3 + k].wait_recv()
        rows = rg[:, zz].reshape(128, 512).astype(F32)
        fk = pl.ds(pl.multiple_of(zz * 512, 512), 512)
        for q in range(4):
            piece = rows[:, q * 128:(q + 1) * 128]
            squares = squares + piece * piece
        lhs = (rows * gain_mlp[:, fk]).astype(BF16)
        for cc in range(2):
            acc[cc] = acc[cc] + jnp.dot(lhs, wup[cc, fk, :], preferred_element_type=F32)
    second_scale = lax.rsqrt(jnp.sum(squares, axis=1, keepdims=True) / 4096.0 + EPS)
    hid = []
    for cc in range(2):
        upper = jnp.maximum(acc[cc] * second_scale, 0.0)
        hid.append((upper * upper).astype(BF16))

    ld_dn.wait()
    mlp_cp[1].wait_recv()
    xs_cp = {}
    bz_cp = {}
    for i in range(NZ):
        dz = (FAR + (0,))[i]
        zz = zp(dz)
        fk = pl.ds(pl.multiple_of(zz * 512, 512), 512)
        part = jnp.dot(hid[0], wdn[0, :, fk], preferred_element_type=F32)
        part = part + jnp.dot(hid[1], wdn[1, :, fk], preferred_element_type=F32)
        part = part.astype(BF16)
        for xx in range(NX):
            xsb[dz, xx] = part[:96, xx * 128:(xx + 1) * 128]
            bzs[dz, xx] = part[96:, xx * 128:(xx + 1) * 128]
        if dz:
            bz_cp[dz] = remote(bzs.at[dz], bzr.at[dz - 1], bz_ss.at[dz], bz_rs.at[dz], {"kv_0": zp(dz)})
        for dx in (2, 1, 3):
            xs_cp[dz, dx] = remote(
                xsb.at[dz, xp(dx)], xrb.at[dz, dx - 1], xs_ss.at[dz, dx], xs_rs.at[dz, dx], {"kv_1": xp(dx)}
            )
    zs_cp = {}
    own_sum = None
    for i in range(NZ):
        dz = (FAR + (0,))[i]
        for dx in (2, 1, 3):
            xs_cp[dz, dx].wait_recv()
        summed = xsb[dz, x].astype(F32) + jnp.sum(xrb[dz].astype(F32), axis=0)
        if dz:
            zsb[dz] = summed.astype(BF16)
            zs_cp[dz] = remote(zsb.at[dz], zrb.at[dz - 1], zs_ss.at[dz], zs_rs.at[dz], {"kv_0": zp(dz)})
        else:
            own_sum = summed
    for dz in FAR:
        bz_cp[dz].wait_recv()
    last = bzs[0].astype(F32) + jnp.sum(bzr[...].astype(F32), axis=0)
    bxs[...] = last.astype(BF16)
    bx_cp = []
    for dx in (2, 1, 3):
        bx_cp.append(
            remote(bxs.at[xp(dx)], bxr.at[dx - 1], bx_ss.at[dx], bx_rs.at[dx], {"kv_1": xp(dx)})
        )
    for dz in FAR:
        zs_cp[dz].wait_recv()
    first = own_sum + jnp.sum(zrb[...].astype(F32), axis=0)
    for cp in bx_cp:
        cp.wait_recv()
    last = bxs[x].astype(F32) + jnp.sum(bxr[...].astype(F32), axis=0)
    down = jnp.concatenate([first, last], axis=0)
    lanes = pl.ds(pl.multiple_of(x * 128, 128), 128)
    res = rg[:, z, :, lanes].reshape(128, 128).astype(F32)
    fsend[...] = (res + down).astype(BF16)
    f_cp = remote(fsend, frecv, f_ss, f_rs, partner)
    f_cp.wait_recv()
    for who, ref in ((c, fsend), (1 - c, frecv)):
        block = ref[...].astype(F32)
        for xs in range(NX):
            for zl in range(4):
                r0 = xs * 32 + zl * 8
                fin[(who * 4 + zl) * NX + xs] = block[r0:r0 + 8]
    fint[...] = jnp.transpose(fin[...].reshape(256, 128))
    out[...] = fint[pl.ds(pl.multiple_of(c * 64, 64), 64), :].astype(BF16)

    for cp in tok_cp + tokp_cp + w_cp[0] + w_cp[1] + w_cp[2] + mlp_cp + ssq_cp + mix_cp + my_cp + h_cp + [pr_cp]:
        cp.wait_send()
    for ch in range(3):
        pltpu.make_async_copy(sbuf.at[ch, 1:32], sbuf.at[ch, 1:32], p1_ss.at[ch]).wait()
    for cp in list(rz_cp.values()) + rx_cp + list(xs_cp.values()) + list(zs_cp.values()) + list(bz_cp.values()) + bx_cp + [f_cp]:
        cp.wait_send()
    for cp in ns_cp:
        cp.wait()


def tail(res_in, state_in, result, new_state, st, res, ld_sem, out_sem):
    moves = [(state_in.at[b], st.at[b], new_state.at[b]) for b in range(8)] + [(res_in, res, result)]
    loads = [pltpu.make_async_copy(src, held, ld_sem.at[i]) for i, (src, held, _) in enumerate(moves)]
    stores = [pltpu.make_async_copy(held, dst, out_sem.at[i]) for i, (_, held, dst) in enumerate(moves)]
    for cp in loads:
        cp.start()
    for i in range(9):
        loads[i].wait()
        stores[i].start()
    for cp in stores:
        cp.wait()


def per_device(
    tokens, gain_mix, gain_mlp, decay_rate, w_query, w_key, w_value, w_gate, w_mix, w_up, w_down, state
):
    vm = pl.BlockSpec(memory_space=pltpu.VMEM)
    sm = pl.BlockSpec(memory_space=pltpu.SMEM)
    hbm = pl.BlockSpec(memory_space=pltpu.HBM)
    dma = pltpu.SemaphoreType.DMA
    state = state.reshape(8, 4, 128, 128)
    result, new_state = pl.pallas_call(
        kernel,
        out_shape=(
            jax.ShapeDtypeStruct((64, 256), BF16),
            jax.ShapeDtypeStruct((8, 4, 128, 128), F32),
        ),
        in_specs=[hbm, hbm, hbm, sm] + [hbm] * 8,
        out_specs=(vm, hbm),
        scratch_shapes=[
            pltpu.VMEM((1, 4096), F32),
            pltpu.VMEM((1, 4096), F32),
            pltpu.VMEM((4, 2, 64, 256), BF16),
            pltpu.VMEM((32, 8, 512), F32),
            pltpu.VMEM((4, 128, 768), BF16),
            pltpu.VMEM((4, 1024, 128), BF16),
            pltpu.VMEM((2, 4096, 256), BF16),
            pltpu.VMEM((2, 256, 4096), BF16),
            pltpu.VMEM((8, 4, 128, 128), F32),
            pltpu.VMEM((3, 32, 16, 128), BF16),
            pltpu.VMEM((3, 32, 16, 128), BF16),
            pltpu.VMEM((32, 8, 128), F32),
            pltpu.VMEM((8, 8, 128), F32),
            pltpu.VMEM((4, 16, 128), F32),
            pltpu.VMEM((4, 16, 128), F32),
            pltpu.VMEM((4, 16, 128), F32),
            pltpu.VMEM((4, 16, 128), F32),
            pltpu.VMEM((8, 4, 16, 128), BF16),
            pltpu.VMEM((2, 32, 512), BF16),
            pltpu.VMEM((32, 512), BF16),
            pltpu.VMEM((4, 8, 32, 512), BF16),
            pltpu.VMEM((8, 4, 96, 128), BF16),
            pltpu.VMEM((8, 3, 96, 128), BF16),
            pltpu.VMEM((8, 96, 128), BF16),
            pltpu.VMEM((7, 96, 128), BF16),
            pltpu.VMEM((8, 4, 32, 128), BF16),
            pltpu.VMEM((7, 4, 32, 128), BF16),
            pltpu.VMEM((4, 32, 128), BF16),
            pltpu.VMEM((3, 32, 128), BF16),
            pltpu.VMEM((128, 128), BF16),
            pltpu.VMEM((128, 128), BF16),
            pltpu.VMEM((32, 8, 128), F32),
            pltpu.VMEM((128, 256), F32),
            dma((11,)), dma((4,)), dma((8,)), dma((8,)), dma((4, 4)), dma((4, 4)), dma((4,)), dma((4,)), dma((4, 4)), dma((4, 4)),
            dma((2,)), dma((2,)), dma((3,)), dma((3,)), dma((8,)), dma((8,)), dma((8,)), dma((8,)),
            dma, dma, dma((8,)), dma((8,)), dma((8, 4)), dma((8, 4)), dma((8, 4)), dma((8, 4)),
            dma((8,)), dma((8,)), dma((8,)), dma((8,)), dma((4,)), dma((4,)), dma, dma,
        ],
        compiler_params=pltpu.CompilerParams(
            collective_id=0, has_side_effects=True, vmem_limit_bytes=60 * 1024 * 1024
        ),
        name="layer",
    )(
        tokens.T, gain_mix.reshape(1, 4096), gain_mlp.reshape(1, 4096), decay_rate,
        w_query, w_key, w_value, w_gate, w_mix, w_up, w_down, state,
    )
    result, new_state = pl.pallas_call(
        tail,
        out_shape=(
            jax.ShapeDtypeStruct((64, 256), BF16),
            jax.ShapeDtypeStruct((8, 4, 128, 128), F32),
        ),
        in_specs=[hbm, hbm],
        out_specs=(hbm, hbm),
        scratch_shapes=[
            pltpu.VMEM((8, 4, 128, 128), F32),
            pltpu.VMEM((64, 256), BF16),
            dma((9,)), dma((9,)),
        ],
        compiler_params=pltpu.CompilerParams(vmem_limit_bytes=60 * 1024 * 1024),
        name="tail",
    )(result, new_state)
    return result.T, new_state.reshape(8, 8, 64, 128)


def solution(mesh):
    torus = Mesh(
        mesh.devices.reshape(mesh.shape["dp"], 8, 4, mesh.shape["tp"]), ("dp", "kv_0", "kv_1", "tp")
    )
    return jax.shard_map(
        per_device,
        mesh=torus,
        in_specs=(
            P("dp", KV_TP),
            P(),
            P(),
            P(),
            P(KV, "tp"),
            P(KV, "tp"),
            P(KV, "tp"),
            P(KV, "tp"),
            P("tp", KV),
            P(None, KV_TP),
            P(KV_TP, None),
            P(DP_KV, "tp", None, None),
        ),
        out_specs=(P("dp", KV_TP), P(DP_KV, "tp", None, None)),
        check_vma=False,
    )
```

```python
import jax
import jax.numpy as jnp
from jax import lax
from jax.sharding import Mesh
from jax.sharding import PartitionSpec as P
from jax.experimental import pallas as pl
from jax.experimental.pallas import tpu as pltpu

KV = ("kv_0", "kv_1")
KV_TP = ("kv_0", "kv_1", "tp")
DP_KV = ("dp", "kv_0", "kv_1")
EPS = 1e-06
F32 = jnp.float32
BF16 = jnp.bfloat16
MESH = pl.DeviceIdType.MESH
NZ = 8
NX = 4
FAR = (4, 3, 5, 2, 6, 1, 7)


def kernel(
    tokens, gain_mix_h, gain_mlp_h, rates_h, w_query, w_key, w_value, w_gate, w_mix, w_up, w_down, state,
    out, new_state,
    gain_mix, gain_mlp, tok_in, tokf, wbuf, wm, wup, wdn, st,
    sbuf, rbuf, ssq_s, ssq_r, qk_abs, v_abs, g_abs, rdbuf, hall, pbuf, pin, rg,
    xsb, xrb, zsb, zrb, bzs, bzr, bxs, bxr, fsend, frecv, fin, fint,
    rates, hop, loc_sem, ns_sem, tok_ss, tok_rs, w_ss, w_rs, mix_ss, mix_rs, my_ss, my_rs, mlp_ss, mlp_rs,
    p1_ss, p1_rs, ssq_ss, ssq_rs, h_ss, h_rs, pr_ss, pr_rs,
    rz_ss, rz_rs, rx_ss, rx_rs, xs_ss, xs_rs, zs_ss, zs_rs, bz_ss, bz_rs, bx_ss, bx_rs, f_ss, f_rs,
):
    z = lax.axis_index("kv_0")
    x = lax.axis_index("kv_1")
    c = lax.axis_index("tp")
    y = lax.axis_index("dp")
    kv = z * NX + x

    def zp(d):
        return lax.rem(z + d, NZ)

    def xp(d):
        return lax.rem(x + d, NX)

    bar = pltpu.get_barrier_semaphore()
    nearby = [{"tp": 1 - c}, {"kv_0": zp(1)}, {"kv_0": zp(NZ - 1)}]
    nearby += [{"kv_1": xp(dx)} for dx in range(1, NX)]
    nearby += [{"dp": lax.rem(y + dy, 4)} for dy in range(1, 4)]
    for dev in nearby:
        pl.semaphore_signal(bar, inc=1, device_id=dev, device_id_type=MESH)

    def local(src, dst, i):
        cp = pltpu.make_async_copy(src, dst, loc_sem.at[i])
        cp.start()
        return cp

    cq = pl.ds(pl.multiple_of(x * 128, 128), 128)
    cv = pl.ds(pl.multiple_of(x * 256, 256), 256)
    ld_tok = local(tokens, tok_in.at[x, c], 8)
    ld_gains = [local(gain_mix_h, gain_mix, 9), local(gain_mlp_h, gain_mlp, 10), local(rates_h, rates, 11)]
    ld_w = [
        local(w_query.at[:, cq], wbuf.at[x, :, 0:128], 0),
        local(w_key.at[:, cq], wbuf.at[x, :, 128:256], 1),
        local(w_value.at[:, cv], wbuf.at[x, :, 256:512], 2),
        local(w_gate.at[:, cv], wbuf.at[x, :, 512:768], 3),
    ]
    ld_st = local(state, st, 4)
    ld_mix = local(w_mix, wm.at[x], 5)
    ld_up = local(w_up, wup.at[c], 6)
    ld_dn = local(w_down, wdn.at[c], 7)

    ld_tok.wait()
    pl.semaphore_wait(bar, len(nearby))

    partner = {"tp": 1 - c}

    def remote(src, dst, ss, rs, dev):
        cp = pltpu.make_async_remote_copy(
            src_ref=src, dst_ref=dst, send_sem=ss, recv_sem=rs, device_id=dev, device_id_type=MESH
        )
        cp.start()
        return cp

    tok_cp = []
    for dx in (2, 1, 3):
        tok_cp.append(
            remote(tok_in.at[x, c], tok_in.at[x, c], tok_ss.at[dx], tok_rs.at[dx], {"kv_1": xp(dx)})
        )
    tokp_cp = [remote(tok_in.at[x, c], tok_in.at[x, c], tok_ss.at[4], tok_rs.at[4], {"tp": 1 - c})]

    w_cp = {0: [], 1: [], 2: []}
    for dx in (2, 1, 3):
        dev = {"kv_1": xp(dx)}
        dq = pl.ds(pl.multiple_of(xp(dx) * 128, 128), 128)
        w_cp[0].append(remote(w_query.at[:, dq], wbuf.at[x, :, 0:128], w_ss.at[0, dx], w_rs.at[0, dx], dev))
        w_cp[0].append(remote(w_key.at[:, dq], wbuf.at[x, :, 128:256], w_ss.at[1, dx], w_rs.at[1, dx], dev))
    for j, (w, lo) in enumerate(((w_value, 256), (w_gate, 512))):
        for dx in (2, 1, 3):
            dev = {"kv_1": xp(dx)}
            dv = pl.ds(pl.multiple_of(xp(dx) * 256, 256), 256)
            w_cp[j + 1].append(
                remote(w.at[:, dv], wbuf.at[x, :, lo:lo + 256], w_ss.at[2 + j, dx], w_rs.at[2 + j, dx], dev)
            )

    qrows = pl.ds(pl.multiple_of(y * 256, 256), 256)
    mix_cp = []
    for dx in (2, 1, 3):
        mix_cp.append(
            remote(w_mix.at[qrows], wm.at[x, qrows], mix_ss.at[dx], mix_rs.at[dx], {"kv_1": xp(dx)})
        )

    for r in range(4):
        pl.semaphore_signal(hop.at[r, 0], inc=1, device_id={"kv_0": zp(1)}, device_id_type=MESH)
        pl.semaphore_signal(hop.at[r, 1], inc=1, device_id={"kv_0": zp(NZ - 1)}, device_id_type=MESH)
        pl.semaphore_wait(hop.at[r, 0], 1)
        pl.semaphore_wait(hop.at[r, 1], 1)

    for i, dx in enumerate((1, 3, 2)):
        tok_cp[(1, 2, 0)[i]].wait_recv()
        src = tok_in.at[xp(NX - dx), c]
        tokp_cp.append(remote(src, src, tok_ss.at[4 + dx], tok_rs.at[4 + dx], {"tp": 1 - c}))
    for cp in tokp_cp:
        cp.wait_recv()
    squares = jnp.zeros((256, 128), F32)
    for xx in range(NX):
        both = jnp.transpose(tok_in[xx].reshape(128, 256).astype(F32))
        tokf[:, :, xx * 128:(xx + 1) * 128] = both.reshape(32, 8, 128)
        squares = squares + both * both
    ssq_s[...] = jnp.broadcast_to(jnp.sum(squares, axis=1, keepdims=True), (256, 128)).reshape(32, 8, 128)
    ssq_cp = []
    for dz in FAR:
        ssq_cp.append(
            remote(ssq_s.at[zp(dz) * NX + x], ssq_r.at[dz], ssq_ss.at[dz], ssq_rs.at[dz], {"kv_0": zp(dz)})
        )
    fz = pl.ds(pl.multiple_of(z * 512, 512), 512)
    for ld in ld_gains:
        ld.wait()
    normed = (tokf[...].reshape(256, 512) * gain_mix[:, fz]).astype(BF16)

    for ch in range(3):
        for cp in w_cp[ch]:
            cp.wait_recv()
        for ld in (ld_w[0:2], ld_w[2:3], ld_w[3:4])[ch]:
            ld.wait()
        wch = wbuf[:, :, ch * 256:(ch + 1) * 256].reshape(512, 256)
        part = jnp.dot(normed, wch, preferred_element_type=F32).reshape(32, 8, 256)
        sbuf[ch] = jnp.concatenate([part[:, :, :128], part[:, :, 128:]], axis=1).astype(BF16)

        def scatter(i, _, ch=ch):
            zz, xx = zp(i // NX), xp(i % NX)
            remote(
                sbuf.at[ch, zz * NX + xx], rbuf.at[ch, i], p1_ss.at[ch], p1_rs.at[ch], {"kv_0": zz, "kv_1": xx}
            )
            return 0

        lax.fori_loop(1, NZ * NX, scatter, 0)

    mlp_cp = [
        remote(w_up, wup.at[c], mlp_ss.at[0], mlp_rs.at[0], partner),
        remote(w_down, wdn.at[c], mlp_ss.at[1], mlp_rs.at[1], partner),
    ]

    my_cp = []
    for i, dx in enumerate((2, 1, 3)):
        mix_cp[i].wait_recv()
        src = wm.at[xp(NX - dx), qrows]
        for dy in (2, 1, 3):
            my_cp.append(remote(src, src, my_ss.at[dx, dy], my_rs.at[dx, dy], {"dp": lax.rem(y + dy, 4)}))

    for cp in ssq_cp:
        cp.wait_recv()
    ssq_r[0] = ssq_s[kv]
    total = jnp.sum(ssq_r[...], axis=0)
    first_scale = lax.rsqrt(total / 4096.0 + EPS)
    scale16 = jnp.concatenate([first_scale, first_scale], axis=0)[None]

    def own(ch):
        pltpu.make_async_copy(rbuf.at[ch, 1:32], rbuf.at[ch, 1:32], p1_rs.at[ch]).wait()
        rbuf[ch, 0] = sbuf[ch, kv]
        summed = jnp.sum(rbuf[ch].astype(F32).reshape(NZ, NX, 16, 128), axis=0)
        return (summed * scale16).astype(BF16).astype(F32)

    qk = own(0)
    for dx in range(NX):
        qk_abs[xp(NX - dx)] = qk[dx]
    vals = own(1)
    for dx in range(NX):
        v_abs[xp(NX - dx)] = vals[dx]
    qs = qk_abs[:, :8].reshape(32, 128)
    ks = qk_abs[:, 8:].reshape(32, 128) * 0.125
    turned = jnp.transpose(jnp.concatenate([qs, ks, jnp.zeros((64, 128), F32)], axis=0))
    ld_st.wait()
    decays = [jnp.exp(-jnp.full((1, 128), rates[c * 8 + h], F32)) for h in range(8)]
    for xs in range(NX):
        for b in range(8):
            for hh in range(2):
                rows = slice(hh * 64, (hh + 1) * 64)
                col = xs * 8 + b
                new = decays[xs * 2 + hh] * st[b, xs, rows, :] + (
                    turned[rows, 32 + col:33 + col] * v_abs[xs, hh * 8 + b:hh * 8 + b + 1, :]
                )
                st[b, xs, rows, :] = new
                rdbuf[xs, hh * 8 + b:hh * 8 + b + 1, :] = jnp.sum(
                    turned[rows, col:col + 1] * new, axis=0, keepdims=True
                )
    ns_cp = []
    for q in range(4):
        cp = pltpu.make_async_copy(st.at[2 * q:2 * q + 2], new_state.at[2 * q:2 * q + 2], ns_sem.at[q])
        cp.start()
        ns_cp.append(cp)
    gates = own(2)
    for dx in range(NX):
        g_abs[xp(NX - dx)] = gates[dx]
    gates = g_abs[...]
    read = rdbuf[...]
    read = read * lax.rsqrt(jnp.mean(read * read, axis=2, keepdims=True) + EPS)
    hall[z] = (gates / (1.0 + jnp.exp(-gates)) * read).astype(BF16)
    h_cp = []
    for dz in FAR:
        h_cp.append(remote(hall.at[z], hall.at[z], h_ss.at[dz], h_rs.at[dz], {"kv_0": zp(dz)}))
    for cp in h_cp:
        cp.wait_recv()
    for cp in my_cp:
        cp.wait_recv()
    ld_mix.wait()

    pieces = []
    for xs in range(NX):
        both = hall[:, xs].astype(F32)
        for hh in range(2):
            pieces.append(both[:, hh * 8:(hh + 1) * 8].reshape(64, 128).astype(BF16))
    lhs = jnp.concatenate(pieces, axis=1)
    for xx in range(NX):
        prod = jnp.dot(lhs, wm[xx], preferred_element_type=F32).astype(BF16)
        pbuf[0, :, xx * 128:(xx + 1) * 128] = prod[:32]
        pbuf[1, :, xx * 128:(xx + 1) * 128] = prod[32:]
    pr_cp = remote(pbuf.at[1 - c], pin, pr_ss, pr_rs, partner)
    pr_cp.wait_recv()
    mixed = pbuf[c].astype(F32) + pin[...].astype(F32)
    own_tok = []
    for zl in range(4):
        own_tok.append(tokf[(c * 4 + zl) * NX + x])
    rg[x, z] = (jnp.concatenate(own_tok, axis=0) + mixed).astype(BF16)

    rz_cp = {}
    for dz in (1, 7, 2, 6, 3, 5, 4):
        rz_cp[dz] = remote(rg.at[x, z], rg.at[x, z], rz_ss.at[dz], rz_rs.at[dz], {"kv_0": zp(dz)})
    rx_cp = []
    ORDER = (0, 1, 7, 2, 6, 3, 5, 4)
    for dz in ORDER:
        zz = lax.rem(z - dz + NZ, NZ)
        if dz:
            rz_cp[dz].wait_recv()
        for dx in (2, 1, 3):
            rx_cp.append(
                remote(rg.at[x, zz], rg.at[x, zz], rx_ss.at[dz, dx], rx_rs.at[dz, dx], {"kv_1": xp(dx)})
            )
    ld_up.wait()
    mlp_cp[0].wait_recv()
    acc = [jnp.zeros((128, 256), F32), jnp.zeros((128, 256), F32)]
    squares = jnp.zeros((128, 128), F32)
    for i, dz in enumerate(ORDER):
        zz = lax.rem(z - dz + NZ, NZ)
        for k in range(3):
            rx_cp[i * 3 + k].wait_recv()
        rows = rg[:, zz].reshape(128, 512).astype(F32)
        fk = pl.ds(pl.multiple_of(zz * 512, 512), 512)
        for q in range(4):
            piece = rows[:, q * 128:(q + 1) * 128]
            squares = squares + piece * piece
        lhs = (rows * gain_mlp[:, fk]).astype(BF16)
        for cc in range(2):
            acc[cc] = acc[cc] + jnp.dot(lhs, wup[cc, fk, :], preferred_element_type=F32)
    second_scale = lax.rsqrt(jnp.sum(squares, axis=1, keepdims=True) / 4096.0 + EPS)
    hid = []
    for cc in range(2):
        upper = jnp.maximum(acc[cc] * second_scale, 0.0)
        hid.append((upper * upper).astype(BF16))

    ld_dn.wait()
    mlp_cp[1].wait_recv()
    xs_cp = {}
    bz_cp = {}
    for i in range(NZ):
        dz = (FAR + (0,))[i]
        zz = zp(dz)
        fk = pl.ds(pl.multiple_of(zz * 512, 512), 512)
        part = jnp.dot(hid[0], wdn[0, :, fk], preferred_element_type=F32)
        part = part + jnp.dot(hid[1], wdn[1, :, fk], preferred_element_type=F32)
        part = part.astype(BF16)
        for xx in range(NX):
            xsb[dz, xx] = part[:96, xx * 128:(xx + 1) * 128]
            bzs[dz, xx] = part[96:, xx * 128:(xx + 1) * 128]
        if dz:
            bz_cp[dz] = remote(bzs.at[dz], bzr.at[dz - 1], bz_ss.at[dz], bz_rs.at[dz], {"kv_0": zp(dz)})
        for dx in (2, 1, 3):
            xs_cp[dz, dx] = remote(
                xsb.at[dz, xp(dx)], xrb.at[dz, dx - 1], xs_ss.at[dz, dx], xs_rs.at[dz, dx], {"kv_1": xp(dx)}
            )
    zs_cp = {}
    own_sum = None
    for i in range(NZ):
        dz = (FAR + (0,))[i]
        for dx in (2, 1, 3):
            xs_cp[dz, dx].wait_recv()
        summed = xsb[dz, x].astype(F32) + jnp.sum(xrb[dz].astype(F32), axis=0)
        if dz:
            zsb[dz] = summed.astype(BF16)
            zs_cp[dz] = remote(zsb.at[dz], zrb.at[dz - 1], zs_ss.at[dz], zs_rs.at[dz], {"kv_0": zp(dz)})
        else:
            own_sum = summed
    for dz in FAR:
        bz_cp[dz].wait_recv()
    last = bzs[0].astype(F32) + jnp.sum(bzr[...].astype(F32), axis=0)
    bxs[...] = last.astype(BF16)
    bx_cp = []
    for dx in (2, 1, 3):
        bx_cp.append(
            remote(bxs.at[xp(dx)], bxr.at[dx - 1], bx_ss.at[dx], bx_rs.at[dx], {"kv_1": xp(dx)})
        )
    for dz in FAR:
        zs_cp[dz].wait_recv()
    first = own_sum + jnp.sum(zrb[...].astype(F32), axis=0)
    for cp in bx_cp:
        cp.wait_recv()
    last = bxs[x].astype(F32) + jnp.sum(bxr[...].astype(F32), axis=0)
    down = jnp.concatenate([first, last], axis=0)
    lanes = pl.ds(pl.multiple_of(x * 128, 128), 128)
    res = rg[:, z, :, lanes].reshape(128, 128).astype(F32)
    fsend[...] = (res + down).astype(BF16)
    f_cp = remote(fsend, frecv, f_ss, f_rs, partner)
    f_cp.wait_recv()
    for who, ref in ((c, fsend), (1 - c, frecv)):
        block = ref[...].astype(F32)
        for xs in range(NX):
            for zl in range(4):
                r0 = xs * 32 + zl * 8
                fin[(who * 4 + zl) * NX + xs] = block[r0:r0 + 8]
    fint[...] = jnp.transpose(fin[...].reshape(256, 128))
    out[...] = fint[pl.ds(pl.multiple_of(c * 64, 64), 64), :].astype(BF16)

    for cp in tok_cp + tokp_cp + w_cp[0] + w_cp[1] + w_cp[2] + mlp_cp + ssq_cp + mix_cp + my_cp + h_cp + [pr_cp]:
        cp.wait_send()
    for ch in range(3):
        pltpu.make_async_copy(sbuf.at[ch, 1:32], sbuf.at[ch, 1:32], p1_ss.at[ch]).wait()
    for cp in list(rz_cp.values()) + rx_cp + list(xs_cp.values()) + list(zs_cp.values()) + list(bz_cp.values()) + bx_cp + [f_cp]:
        cp.wait_send()
    for cp in ns_cp:
        cp.wait()


def tail(res_in, state_in, result, new_state, st, res, ld_sem, out_sem):
    moves = [(state_in.at[b], st.at[b], new_state.at[b]) for b in range(8)] + [(res_in, res, result)]
    loads = [pltpu.make_async_copy(src, held, ld_sem.at[i]) for i, (src, held, _) in enumerate(moves)]
    stores = [pltpu.make_async_copy(held, dst, out_sem.at[i]) for i, (_, held, dst) in enumerate(moves)]
    for cp in loads:
        cp.start()
    for i in range(9):
        loads[i].wait()
        stores[i].start()
    for cp in stores:
        cp.wait()


def per_device(
    tokens, gain_mix, gain_mlp, decay_rate, w_query, w_key, w_value, w_gate, w_mix, w_up, w_down, state
):
    vm = pl.BlockSpec(memory_space=pltpu.VMEM)
    hbm = pl.BlockSpec(memory_space=pltpu.HBM)
    dma = pltpu.SemaphoreType.DMA
    state = state.reshape(8, 4, 128, 128)
    result, new_state = pl.pallas_call(
        kernel,
        out_shape=(
            jax.ShapeDtypeStruct((64, 256), BF16),
            jax.ShapeDtypeStruct((8, 4, 128, 128), F32),
        ),
        in_specs=[hbm] * 12,
        out_specs=(vm, hbm),
        scratch_shapes=[
            pltpu.VMEM((1, 4096), F32),
            pltpu.VMEM((1, 4096), F32),
            pltpu.VMEM((4, 2, 64, 256), BF16),
            pltpu.VMEM((32, 8, 512), F32),
            pltpu.VMEM((4, 128, 768), BF16),
            pltpu.VMEM((4, 1024, 128), BF16),
            pltpu.VMEM((2, 4096, 256), BF16),
            pltpu.VMEM((2, 256, 4096), BF16),
            pltpu.VMEM((8, 4, 128, 128), F32),
            pltpu.VMEM((3, 32, 16, 128), BF16),
            pltpu.VMEM((3, 32, 16, 128), BF16),
            pltpu.VMEM((32, 8, 128), F32),
            pltpu.VMEM((8, 8, 128), F32),
            pltpu.VMEM((4, 16, 128), F32),
            pltpu.VMEM((4, 16, 128), F32),
            pltpu.VMEM((4, 16, 128), F32),
            pltpu.VMEM((4, 16, 128), F32),
            pltpu.VMEM((8, 4, 16, 128), BF16),
            pltpu.VMEM((2, 32, 512), BF16),
            pltpu.VMEM((32, 512), BF16),
            pltpu.VMEM((4, 8, 32, 512), BF16),
            pltpu.VMEM((8, 4, 96, 128), BF16),
            pltpu.VMEM((8, 3, 96, 128), BF16),
            pltpu.VMEM((8, 96, 128), BF16),
            pltpu.VMEM((7, 96, 128), BF16),
            pltpu.VMEM((8, 4, 32, 128), BF16),
            pltpu.VMEM((7, 4, 32, 128), BF16),
            pltpu.VMEM((4, 32, 128), BF16),
            pltpu.VMEM((3, 32, 128), BF16),
            pltpu.VMEM((128, 128), BF16),
            pltpu.VMEM((128, 128), BF16),
            pltpu.VMEM((32, 8, 128), F32),
            pltpu.VMEM((128, 256), F32),
            pltpu.SMEM((16,), F32), pltpu.SemaphoreType.REGULAR((4, 2)), dma((12,)), dma((4,)), dma((8,)), dma((8,)), dma((4, 4)), dma((4, 4)), dma((4,)), dma((4,)), dma((4, 4)), dma((4, 4)),
            dma((2,)), dma((2,)), dma((3,)), dma((3,)), dma((8,)), dma((8,)), dma((8,)), dma((8,)),
            dma, dma, dma((8,)), dma((8,)), dma((8, 4)), dma((8, 4)), dma((8, 4)), dma((8, 4)),
            dma((8,)), dma((8,)), dma((8,)), dma((8,)), dma((4,)), dma((4,)), dma, dma,
        ],
        compiler_params=pltpu.CompilerParams(
            collective_id=0, has_side_effects=True, vmem_limit_bytes=60 * 1024 * 1024
        ),
        name="layer",
    )(
        tokens.T, gain_mix.reshape(1, 4096), gain_mlp.reshape(1, 4096), decay_rate,
        w_query, w_key, w_value, w_gate, w_mix, w_up, w_down, state,
    )
    result, new_state = pl.pallas_call(
        tail,
        out_shape=(
            jax.ShapeDtypeStruct((64, 256), BF16),
            jax.ShapeDtypeStruct((8, 4, 128, 128), F32),
        ),
        in_specs=[hbm, hbm],
        out_specs=(hbm, hbm),
        scratch_shapes=[
            pltpu.VMEM((8, 4, 128, 128), F32),
            pltpu.VMEM((64, 256), BF16),
            dma((9,)), dma((9,)),
        ],
        compiler_params=pltpu.CompilerParams(vmem_limit_bytes=60 * 1024 * 1024),
        name="tail",
    )(result, new_state)
    return result.T, new_state.reshape(8, 8, 64, 128)


def solution(mesh):
    torus = Mesh(
        mesh.devices.reshape(mesh.shape["dp"], 8, 4, mesh.shape["tp"]), ("dp", "kv_0", "kv_1", "tp")
    )
    return jax.shard_map(
        per_device,
        mesh=torus,
        in_specs=(
            P("dp", KV_TP),
            P(),
            P(),
            P(),
            P(KV, "tp"),
            P(KV, "tp"),
            P(KV, "tp"),
            P(KV, "tp"),
            P("tp", KV),
            P(None, KV_TP),
            P(KV_TP, None),
            P(DP_KV, "tp", None, None),
        ),
        out_specs=(P("dp", KV_TP), P(DP_KV, "tp", None, None)),
        check_vma=False,
    )
```

```python
import jax
import jax.numpy as jnp
from jax import lax
from jax.sharding import Mesh
from jax.sharding import PartitionSpec as P
from jax.experimental import pallas as pl
from jax.experimental.pallas import tpu as pltpu

KV = ("kv_0", "kv_1")
KV_TP = ("kv_0", "kv_1", "tp")
DP_KV = ("dp", "kv_0", "kv_1")
EPS = 1e-06
F32 = jnp.float32
BF16 = jnp.bfloat16
MESH = pl.DeviceIdType.MESH
NZ = 8
NX = 4
FAR = (4, 3, 5, 2, 6, 1, 7)


def kernel(
    tokens, gain_mix_h, gain_mlp_h, rates_h, w_query, w_key, w_value, w_gate, w_mix, w_up, w_down, state,
    out, new_state,
    gain_mix, gain_mlp, tok_in, tokf, wbuf, wm, wup, wdn, st,
    sbuf, rbuf, ssq_s, ssq_r, qk_abs, v_abs, g_abs, rdbuf, hall, pbuf, pin, rg,
    xsb, xrb, zsb, zrb, bzs, bzr, bxs, bxr, fsend, frecv, fin, fint,
    rates, hop, loc_sem, ns_sem, tok_ss, tok_rs, w_ss, w_rs, mix_ss, mix_rs, my_ss, my_rs, mlp_ss, mlp_rs,
    p1_ss, p1_rs, ssq_ss, ssq_rs, h_ss, h_rs, pr_ss, pr_rs,
    rz_ss, rz_rs, rx_ss, rx_rs, xs_ss, xs_rs, zs_ss, zs_rs, bz_ss, bz_rs, bx_ss, bx_rs, f_ss, f_rs,
):
    z = lax.axis_index("kv_0")
    x = lax.axis_index("kv_1")
    c = lax.axis_index("tp")
    y = lax.axis_index("dp")
    kv = z * NX + x

    def zp(d):
        return lax.rem(z + d, NZ)

    def xp(d):
        return lax.rem(x + d, NX)

    bar = pltpu.get_barrier_semaphore()
    nearby = [{"tp": 1 - c}, {"kv_0": zp(1)}, {"kv_0": zp(NZ - 1)}]
    nearby += [{"kv_1": xp(dx)} for dx in range(1, NX)]
    nearby += [{"dp": lax.rem(y + dy, 4)} for dy in range(1, 4)]
    for dev in nearby:
        pl.semaphore_signal(bar, inc=1, device_id=dev, device_id_type=MESH)

    def local(src, dst, i):
        cp = pltpu.make_async_copy(src, dst, loc_sem.at[i])
        cp.start()
        return cp

    cq = pl.ds(pl.multiple_of(x * 128, 128), 128)
    cv = pl.ds(pl.multiple_of(x * 256, 256), 256)
    ld_tok = local(tokens, tok_in.at[x, c], 8)
    ld_gains = [local(gain_mix_h, gain_mix, 9), local(gain_mlp_h, gain_mlp, 10), local(rates_h, rates, 11)]
    ld_w = [
        local(w_query.at[:, cq], wbuf.at[x, :, 0:128], 0),
        local(w_key.at[:, cq], wbuf.at[x, :, 128:256], 1),
        local(w_value.at[:, cv], wbuf.at[x, :, 256:512], 2),
        local(w_gate.at[:, cv], wbuf.at[x, :, 512:768], 3),
    ]
    ld_st = local(state, st, 4)
    ld_mix = local(w_mix, wm.at[x], 5)
    ld_up = local(w_up, wup.at[c], 6)
    ld_dn = local(w_down, wdn.at[c], 7)

    ld_tok.wait()
    pl.semaphore_wait(bar, len(nearby))

    partner = {"tp": 1 - c}

    def remote(src, dst, ss, rs, dev):
        cp = pltpu.make_async_remote_copy(
            src_ref=src, dst_ref=dst, send_sem=ss, recv_sem=rs, device_id=dev, device_id_type=MESH
        )
        cp.start()
        return cp

    tok_cp = []
    for dx in (2, 1, 3):
        tok_cp.append(
            remote(tok_in.at[x, c], tok_in.at[x, c], tok_ss.at[dx], tok_rs.at[dx], {"kv_1": xp(dx)})
        )
    tokp_cp = [remote(tok_in.at[x, c], tok_in.at[x, c], tok_ss.at[4], tok_rs.at[4], {"tp": 1 - c})]

    w_cp = {0: [], 1: [], 2: []}
    for dx in (2, 1, 3):
        dev = {"kv_1": xp(dx)}
        dq = pl.ds(pl.multiple_of(xp(dx) * 128, 128), 128)
        w_cp[0].append(remote(w_query.at[:, dq], wbuf.at[x, :, 0:128], w_ss.at[0, dx], w_rs.at[0, dx], dev))
        w_cp[0].append(remote(w_key.at[:, dq], wbuf.at[x, :, 128:256], w_ss.at[1, dx], w_rs.at[1, dx], dev))
    for j, (w, lo) in enumerate(((w_value, 256), (w_gate, 512))):
        for dx in (2, 1, 3):
            dev = {"kv_1": xp(dx)}
            dv = pl.ds(pl.multiple_of(xp(dx) * 256, 256), 256)
            w_cp[j + 1].append(
                remote(w.at[:, dv], wbuf.at[x, :, lo:lo + 256], w_ss.at[2 + j, dx], w_rs.at[2 + j, dx], dev)
            )

    qrows = pl.ds(pl.multiple_of(y * 256, 256), 256)
    mix_cp = []
    for dx in (2, 1, 3):
        mix_cp.append(
            remote(w_mix.at[qrows], wm.at[x, qrows], mix_ss.at[dx], mix_rs.at[dx], {"kv_1": xp(dx)})
        )

    for r in range(4):
        pl.semaphore_signal(hop.at[r, 0], inc=1, device_id={"kv_0": zp(1)}, device_id_type=MESH)
        pl.semaphore_signal(hop.at[r, 1], inc=1, device_id={"kv_0": zp(NZ - 1)}, device_id_type=MESH)
        pl.semaphore_wait(hop.at[r, 0], 1)
        pl.semaphore_wait(hop.at[r, 1], 1)

    for i, dx in enumerate((1, 3, 2)):
        tok_cp[(1, 2, 0)[i]].wait_recv()
        src = tok_in.at[xp(NX - dx), c]
        tokp_cp.append(remote(src, src, tok_ss.at[4 + dx], tok_rs.at[4 + dx], {"tp": 1 - c}))
    for cp in tokp_cp:
        cp.wait_recv()
    squares = jnp.zeros((256, 128), F32)
    for xx in range(NX):
        both = jnp.transpose(tok_in[xx].reshape(128, 256).astype(F32))
        tokf[:, :, xx * 128:(xx + 1) * 128] = both.reshape(32, 8, 128)
        squares = squares + both * both
    ssq_s[...] = jnp.broadcast_to(jnp.sum(squares, axis=1, keepdims=True), (256, 128)).reshape(32, 8, 128)
    ssq_cp = []
    for dz in FAR:
        ssq_cp.append(
            remote(ssq_s.at[zp(dz) * NX + x], ssq_r.at[dz], ssq_ss.at[dz], ssq_rs.at[dz], {"kv_0": zp(dz)})
        )
    fz = pl.ds(pl.multiple_of(z * 512, 512), 512)
    for ld in ld_gains:
        ld.wait()
    normed = (tokf[...].reshape(256, 512) * gain_mix[:, fz]).astype(BF16)

    for ch in range(3):
        for cp in w_cp[ch]:
            cp.wait_recv()
        for ld in (ld_w[0:2], ld_w[2:3], ld_w[3:4])[ch]:
            ld.wait()
        wch = wbuf[:, :, ch * 256:(ch + 1) * 256].reshape(512, 256)
        part = jnp.dot(normed, wch, preferred_element_type=F32).reshape(32, 8, 256)
        sbuf[ch] = jnp.concatenate([part[:, :, :128], part[:, :, 128:]], axis=1).astype(BF16)

        def scatter(i, _, ch=ch):
            j, k = i // NX, i % NX
            dz = lax.rem(4 + ((j + 1) // 2) * (1 - 2 * (j % 2)), NZ)
            dx = lax.rem(2 + ((k + 1) // 2) * (1 - 2 * (k % 2)), NX)
            zz, xx = zp(dz), xp(dx)
            remote(
                sbuf.at[ch, zz * NX + xx], rbuf.at[ch, dz * NX + dx], p1_ss.at[ch], p1_rs.at[ch], {"kv_0": zz, "kv_1": xx}
            )
            return 0

        lax.fori_loop(0, NZ * NX - 1, scatter, 0)

    mlp_cp = [
        remote(w_up, wup.at[c], mlp_ss.at[0], mlp_rs.at[0], partner),
        remote(w_down, wdn.at[c], mlp_ss.at[1], mlp_rs.at[1], partner),
    ]

    my_cp = []
    for i, dx in enumerate((2, 1, 3)):
        mix_cp[i].wait_recv()
        src = wm.at[xp(NX - dx), qrows]
        for dy in (2, 1, 3):
            my_cp.append(remote(src, src, my_ss.at[dx, dy], my_rs.at[dx, dy], {"dp": lax.rem(y + dy, 4)}))

    for cp in ssq_cp:
        cp.wait_recv()
    ssq_r[0] = ssq_s[kv]
    total = jnp.sum(ssq_r[...], axis=0)
    first_scale = lax.rsqrt(total / 4096.0 + EPS)
    scale16 = jnp.concatenate([first_scale, first_scale], axis=0)[None]

    def own(ch):
        pltpu.make_async_copy(rbuf.at[ch, 1:32], rbuf.at[ch, 1:32], p1_rs.at[ch]).wait()
        rbuf[ch, 0] = sbuf[ch, kv]
        summed = jnp.sum(rbuf[ch].astype(F32).reshape(NZ, NX, 16, 128), axis=0)
        return (summed * scale16).astype(BF16).astype(F32)

    qk = own(0)
    for dx in range(NX):
        qk_abs[xp(NX - dx)] = qk[dx]
    vals = own(1)
    for dx in range(NX):
        v_abs[xp(NX - dx)] = vals[dx]
    qs = qk_abs[:, :8].reshape(32, 128)
    ks = qk_abs[:, 8:].reshape(32, 128) * 0.125
    turned = jnp.transpose(jnp.concatenate([qs, ks, jnp.zeros((64, 128), F32)], axis=0))
    ld_st.wait()
    decays = [jnp.exp(-jnp.full((1, 128), rates[c * 8 + h], F32)) for h in range(8)]
    for xs in range(NX):
        for b in range(8):
            for hh in range(2):
                rows = slice(hh * 64, (hh + 1) * 64)
                col = xs * 8 + b
                new = decays[xs * 2 + hh] * st[b, xs, rows, :] + (
                    turned[rows, 32 + col:33 + col] * v_abs[xs, hh * 8 + b:hh * 8 + b + 1, :]
                )
                st[b, xs, rows, :] = new
                rdbuf[xs, hh * 8 + b:hh * 8 + b + 1, :] = jnp.sum(
                    turned[rows, col:col + 1] * new, axis=0, keepdims=True
                )
    ns_cp = []
    for q in range(4):
        cp = pltpu.make_async_copy(st.at[2 * q:2 * q + 2], new_state.at[2 * q:2 * q + 2], ns_sem.at[q])
        cp.start()
        ns_cp.append(cp)
    gates = own(2)
    for dx in range(NX):
        g_abs[xp(NX - dx)] = gates[dx]
    gates = g_abs[...]
    read = rdbuf[...]
    read = read * lax.rsqrt(jnp.mean(read * read, axis=2, keepdims=True) + EPS)
    hall[z] = (gates / (1.0 + jnp.exp(-gates)) * read).astype(BF16)
    h_cp = []
    for dz in FAR:
        h_cp.append(remote(hall.at[z], hall.at[z], h_ss.at[dz], h_rs.at[dz], {"kv_0": zp(dz)}))
    for cp in h_cp:
        cp.wait_recv()
    for cp in my_cp:
        cp.wait_recv()
    ld_mix.wait()

    pieces = []
    for xs in range(NX):
        both = hall[:, xs].astype(F32)
        for hh in range(2):
            pieces.append(both[:, hh * 8:(hh + 1) * 8].reshape(64, 128).astype(BF16))
    lhs = jnp.concatenate(pieces, axis=1)
    for xx in range(NX):
        prod = jnp.dot(lhs, wm[xx], preferred_element_type=F32).astype(BF16)
        pbuf[0, :, xx * 128:(xx + 1) * 128] = prod[:32]
        pbuf[1, :, xx * 128:(xx + 1) * 128] = prod[32:]
    pr_cp = remote(pbuf.at[1 - c], pin, pr_ss, pr_rs, partner)
    pr_cp.wait_recv()
    mixed = pbuf[c].astype(F32) + pin[...].astype(F32)
    own_tok = []
    for zl in range(4):
        own_tok.append(tokf[(c * 4 + zl) * NX + x])
    rg[x, z] = (jnp.concatenate(own_tok, axis=0) + mixed).astype(BF16)

    rz_cp = {}
    for dz in (1, 7, 2, 6, 3, 5, 4):
        rz_cp[dz] = remote(rg.at[x, z], rg.at[x, z], rz_ss.at[dz], rz_rs.at[dz], {"kv_0": zp(dz)})
    rx_cp = []
    ORDER = (0, 1, 7, 2, 6, 3, 5, 4)
    for dz in ORDER:
        zz = lax.rem(z - dz + NZ, NZ)
        if dz:
            rz_cp[dz].wait_recv()
        for dx in (2, 1, 3):
            rx_cp.append(
                remote(rg.at[x, zz], rg.at[x, zz], rx_ss.at[dz, dx], rx_rs.at[dz, dx], {"kv_1": xp(dx)})
            )
    ld_up.wait()
    mlp_cp[0].wait_recv()
    acc = [jnp.zeros((128, 256), F32), jnp.zeros((128, 256), F32)]
    squares = jnp.zeros((128, 128), F32)
    for i, dz in enumerate(ORDER):
        zz = lax.rem(z - dz + NZ, NZ)
        for k in range(3):
            rx_cp[i * 3 + k].wait_recv()
        rows = rg[:, zz].reshape(128, 512).astype(F32)
        fk = pl.ds(pl.multiple_of(zz * 512, 512), 512)
        for q in range(4):
            piece = rows[:, q * 128:(q + 1) * 128]
            squares = squares + piece * piece
        lhs = (rows * gain_mlp[:, fk]).astype(BF16)
        for cc in range(2):
            acc[cc] = acc[cc] + jnp.dot(lhs, wup[cc, fk, :], preferred_element_type=F32)
    second_scale = lax.rsqrt(jnp.sum(squares, axis=1, keepdims=True) / 4096.0 + EPS)
    hid = []
    for cc in range(2):
        upper = jnp.maximum(acc[cc] * second_scale, 0.0)
        hid.append((upper * upper).astype(BF16))

    ld_dn.wait()
    mlp_cp[1].wait_recv()
    xs_cp = {}
    bz_cp = {}
    for i in range(NZ):
        dz = (FAR + (0,))[i]
        zz = zp(dz)
        fk = pl.ds(pl.multiple_of(zz * 512, 512), 512)
        part = jnp.dot(hid[0], wdn[0, :, fk], preferred_element_type=F32)
        part = part + jnp.dot(hid[1], wdn[1, :, fk], preferred_element_type=F32)
        part = part.astype(BF16)
        for xx in range(NX):
            xsb[dz, xx] = part[:96, xx * 128:(xx + 1) * 128]
            bzs[dz, xx] = part[96:, xx * 128:(xx + 1) * 128]
        if dz:
            bz_cp[dz] = remote(bzs.at[dz], bzr.at[dz - 1], bz_ss.at[dz], bz_rs.at[dz], {"kv_0": zp(dz)})
        for dx in (2, 1, 3):
            xs_cp[dz, dx] = remote(
                xsb.at[dz, xp(dx)], xrb.at[dz, dx - 1], xs_ss.at[dz, dx], xs_rs.at[dz, dx], {"kv_1": xp(dx)}
            )
    zs_cp = {}
    own_sum = None
    for i in range(NZ):
        dz = (FAR + (0,))[i]
        for dx in (2, 1, 3):
            xs_cp[dz, dx].wait_recv()
        summed = xsb[dz, x].astype(F32) + jnp.sum(xrb[dz].astype(F32), axis=0)
        if dz:
            zsb[dz] = summed.astype(BF16)
            zs_cp[dz] = remote(zsb.at[dz], zrb.at[dz - 1], zs_ss.at[dz], zs_rs.at[dz], {"kv_0": zp(dz)})
        else:
            own_sum = summed
    for dz in FAR:
        bz_cp[dz].wait_recv()
    last = bzs[0].astype(F32) + jnp.sum(bzr[...].astype(F32), axis=0)
    bxs[...] = last.astype(BF16)
    bx_cp = []
    for dx in (2, 1, 3):
        bx_cp.append(
            remote(bxs.at[xp(dx)], bxr.at[dx - 1], bx_ss.at[dx], bx_rs.at[dx], {"kv_1": xp(dx)})
        )
    for dz in FAR:
        zs_cp[dz].wait_recv()
    first = own_sum + jnp.sum(zrb[...].astype(F32), axis=0)
    for cp in bx_cp:
        cp.wait_recv()
    last = bxs[x].astype(F32) + jnp.sum(bxr[...].astype(F32), axis=0)
    down = jnp.concatenate([first, last], axis=0)
    lanes = pl.ds(pl.multiple_of(x * 128, 128), 128)
    res = rg[:, z, :, lanes].reshape(128, 128).astype(F32)
    fsend[...] = (res + down).astype(BF16)
    f_cp = remote(fsend, frecv, f_ss, f_rs, partner)
    f_cp.wait_recv()
    for who, ref in ((c, fsend), (1 - c, frecv)):
        block = ref[...].astype(F32)
        for xs in range(NX):
            for zl in range(4):
                r0 = xs * 32 + zl * 8
                fin[(who * 4 + zl) * NX + xs] = block[r0:r0 + 8]
    fint[...] = jnp.transpose(fin[...].reshape(256, 128))
    out[...] = fint[pl.ds(pl.multiple_of(c * 64, 64), 64), :].astype(BF16)

    for cp in tok_cp + tokp_cp + w_cp[0] + w_cp[1] + w_cp[2] + mlp_cp + ssq_cp + mix_cp + my_cp + h_cp + [pr_cp]:
        cp.wait_send()
    for ch in range(3):
        pltpu.make_async_copy(sbuf.at[ch, 1:32], sbuf.at[ch, 1:32], p1_ss.at[ch]).wait()
    for cp in list(rz_cp.values()) + rx_cp + list(xs_cp.values()) + list(zs_cp.values()) + list(bz_cp.values()) + bx_cp + [f_cp]:
        cp.wait_send()
    for cp in ns_cp:
        cp.wait()


def tail(res_in, state_in, result, new_state, st, res, ld_sem, out_sem):
    moves = [(state_in.at[b], st.at[b], new_state.at[b]) for b in range(8)] + [(res_in, res, result)]
    loads = [pltpu.make_async_copy(src, held, ld_sem.at[i]) for i, (src, held, _) in enumerate(moves)]
    stores = [pltpu.make_async_copy(held, dst, out_sem.at[i]) for i, (_, held, dst) in enumerate(moves)]
    for cp in loads:
        cp.start()
    for i in range(9):
        loads[i].wait()
        stores[i].start()
    for cp in stores:
        cp.wait()


def per_device(
    tokens, gain_mix, gain_mlp, decay_rate, w_query, w_key, w_value, w_gate, w_mix, w_up, w_down, state
):
    vm = pl.BlockSpec(memory_space=pltpu.VMEM)
    hbm = pl.BlockSpec(memory_space=pltpu.HBM)
    dma = pltpu.SemaphoreType.DMA
    state = state.reshape(8, 4, 128, 128)
    result, new_state = pl.pallas_call(
        kernel,
        out_shape=(
            jax.ShapeDtypeStruct((64, 256), BF16),
            jax.ShapeDtypeStruct((8, 4, 128, 128), F32),
        ),
        in_specs=[hbm] * 12,
        out_specs=(vm, hbm),
        scratch_shapes=[
            pltpu.VMEM((1, 4096), F32),
            pltpu.VMEM((1, 4096), F32),
            pltpu.VMEM((4, 2, 64, 256), BF16),
            pltpu.VMEM((32, 8, 512), F32),
            pltpu.VMEM((4, 128, 768), BF16),
            pltpu.VMEM((4, 1024, 128), BF16),
            pltpu.VMEM((2, 4096, 256), BF16),
            pltpu.VMEM((2, 256, 4096), BF16),
            pltpu.VMEM((8, 4, 128, 128), F32),
            pltpu.VMEM((3, 32, 16, 128), BF16),
            pltpu.VMEM((3, 32, 16, 128), BF16),
            pltpu.VMEM((32, 8, 128), F32),
            pltpu.VMEM((8, 8, 128), F32),
            pltpu.VMEM((4, 16, 128), F32),
            pltpu.VMEM((4, 16, 128), F32),
            pltpu.VMEM((4, 16, 128), F32),
            pltpu.VMEM((4, 16, 128), F32),
            pltpu.VMEM((8, 4, 16, 128), BF16),
            pltpu.VMEM((2, 32, 512), BF16),
            pltpu.VMEM((32, 512), BF16),
            pltpu.VMEM((4, 8, 32, 512), BF16),
            pltpu.VMEM((8, 4, 96, 128), BF16),
            pltpu.VMEM((8, 3, 96, 128), BF16),
            pltpu.VMEM((8, 96, 128), BF16),
            pltpu.VMEM((7, 96, 128), BF16),
            pltpu.VMEM((8, 4, 32, 128), BF16),
            pltpu.VMEM((7, 4, 32, 128), BF16),
            pltpu.VMEM((4, 32, 128), BF16),
            pltpu.VMEM((3, 32, 128), BF16),
            pltpu.VMEM((128, 128), BF16),
            pltpu.VMEM((128, 128), BF16),
            pltpu.VMEM((32, 8, 128), F32),
            pltpu.VMEM((128, 256), F32),
            pltpu.SMEM((16,), F32), pltpu.SemaphoreType.REGULAR((4, 2)), dma((12,)), dma((4,)), dma((8,)), dma((8,)), dma((4, 4)), dma((4, 4)), dma((4,)), dma((4,)), dma((4, 4)), dma((4, 4)),
            dma((2,)), dma((2,)), dma((3,)), dma((3,)), dma((8,)), dma((8,)), dma((8,)), dma((8,)),
            dma, dma, dma((8,)), dma((8,)), dma((8, 4)), dma((8, 4)), dma((8, 4)), dma((8, 4)),
            dma((8,)), dma((8,)), dma((8,)), dma((8,)), dma((4,)), dma((4,)), dma, dma,
        ],
        compiler_params=pltpu.CompilerParams(
            collective_id=0, has_side_effects=True, vmem_limit_bytes=60 * 1024 * 1024
        ),
        name="layer",
    )(
        tokens.T, gain_mix.reshape(1, 4096), gain_mlp.reshape(1, 4096), decay_rate,
        w_query, w_key, w_value, w_gate, w_mix, w_up, w_down, state,
    )
    result, new_state = pl.pallas_call(
        tail,
        out_shape=(
            jax.ShapeDtypeStruct((64, 256), BF16),
            jax.ShapeDtypeStruct((8, 4, 128, 128), F32),
        ),
        in_specs=[hbm, hbm],
        out_specs=(hbm, hbm),
        scratch_shapes=[
            pltpu.VMEM((8, 4, 128, 128), F32),
            pltpu.VMEM((64, 256), BF16),
            dma((9,)), dma((9,)),
        ],
        compiler_params=pltpu.CompilerParams(vmem_limit_bytes=60 * 1024 * 1024),
        name="tail",
    )(result, new_state)
    return result.T, new_state.reshape(8, 8, 64, 128)


def solution(mesh):
    torus = Mesh(
        mesh.devices.reshape(mesh.shape["dp"], 8, 4, mesh.shape["tp"]), ("dp", "kv_0", "kv_1", "tp")
    )
    return jax.shard_map(
        per_device,
        mesh=torus,
        in_specs=(
            P("dp", KV_TP),
            P(),
            P(),
            P(),
            P(KV, "tp"),
            P(KV, "tp"),
            P(KV, "tp"),
            P(KV, "tp"),
            P("tp", KV),
            P(None, KV_TP),
            P(KV_TP, None),
            P(DP_KV, "tp", None, None),
        ),
        out_specs=(P("dp", KV_TP), P(DP_KV, "tp", None, None)),
        check_vma=False,
    )
```
